256 devices in a mesh: ep: 16 (over y, x), tp: 16 (over z, core).
Axes of the slice: x: 4, y: 4, z: 8, core: 2. Of those that a mesh axis runs over, the one named last changes fastest.
Arguments:
- tokens: bfloat16 [256, 2048], P('ep'), may hold values from -6 to 6
- norm_gain: float32 [2048], replicated, may hold values from 0.1 to 1.9
- w_query: bfloat16 [2048, 2048], P(None, 'tp'), may hold values from -0.125 to 0.125
- w_key: bfloat16 [2048, 2048], P(None, 'tp'), may hold values from -0.125 to 0.125
- w_value: bfloat16 [2048, 2048], P(None, 'tp'), may hold values from -0.125 to 0.125
- query_gain: float32 [128], replicated, may hold values from 0.1 to 1.9
- key_gain: float32 [128], replicated, may hold values from 0.1 to 1.9
- score_bias: float32 [16], P('tp'), may hold values from -11 to -3.5
- key_cache: bfloat16 [256, 1024, 2048], P('ep', None, 'tp'), may hold values from -6 to 6
- value_cache: bfloat16 [256, 1024, 2048], P('ep', None, 'tp'), may hold values from -6 to 6
- lengths: int32 [256], P('ep'), may hold values from 128 to 1024
- w_out: bfloat16 [2048, 2048], P('tp'), may hold values from -0.125 to 0.125
- post_gain: float32 [2048], replicated, may hold values from 0.1 to 1.9
- routes: int32 [256, 6], P('ep'), may hold values from 0 to 63, all different within a row; in each aligned block of 16 rows (0 to 15, 16 to 31, ...) at most 3 rows name the same one
- route_weight: float32 [256, 6], P('ep'), may hold values from 0.25 to 2
- expert_gate: bfloat16 [256, 2048, 128], P(('ep', 'tp')), may hold values from -0.125 to 0.125
- expert_up: bfloat16 [256, 2048, 128], P(('ep', 'tp')), may hold values from -0.125 to 0.125
- expert_down: bfloat16 [256, 128, 2048], P(('ep', 'tp')), may hold values from -0.25 to 0.25
- shared_gate: bfloat16 [2048, 512], P(None, 'tp'), may hold values from -0.125 to 0.125
- shared_up: bfloat16 [2048, 512], P(None, 'tp'), may hold values from -0.125 to 0.125
- shared_down: bfloat16 [512, 2048], P('tp'), may hold values from -0.25 to 0.25
Outputs:
- mixed: bfloat16 [256, 2048], P('ep', 'tp')
- new_keys: bfloat16 [256, 2048], P('ep', 'tp')
- new_values: bfloat16 [256, 2048], P('ep', 'tp')
The draws below stay inside these ranges and needn't reach their ends.
Inputs may be any that keep to these rules, and one draw needn't show every extreme that they name: `routes`: within the rows of one device no expert is named by more than 3 rows, a bound that some block reaches of them.
All inputs are finite; a program needn't handle non-finite values.
Results may differ from the reference program's by a relative error of at most 0.008.
Values may be sent and summed in bfloat16 or wider, within the bound.
No kernel may reach another device: no remote copies, remote signals or barrier semaphores. Data moves between devices by JAX's collectives and lax.ppermute only.
A program may use at most 64 MiB of HBM per device.

```python
import math
import jax
import jax.numpy as jnp
import numpy as np
from jax import lax

D = 2048
HEADS = 16
HEAD_DIM = 128
EXPERT_DIM = 512
SHARED_DIM = 512
TOPK = 6
SEQ_DEV = 16
CACHE_LEN = 1024
SEQS = 256
EXPERTS = 64
CAP = 3


def draw_score_bias(key, part):
    values = jax.random.uniform(key, (HEADS,), jnp.float32, -9.0, -3.5)
    return values


def with_ends(entries, rng, least, top_value):
    longest = entries.shape.index(max(entries.shape))
    spots = []
    for shift in (0, 1):
        where = [jax.random.randint(jax.random.fold_in(rng, axis), (), 0, length) for axis, length in enumerate(entries.shape)]
        where[longest] = (where[longest] + shift) % entries.shape[longest]
        spots.append(tuple(where))
    return entries.at[spots[0]].set(least).at[spots[1]].set(top_value)


def level_of(rng, shape, split, least, largest):
    level = 1.0
    for axis_at, parts in split:
        steps = jax.random.uniform(jax.random.fold_in(jax.random.fold_in(rng, 6), axis_at), (parts,), jnp.float32, least / len(split), largest / len(split))
        level = level * jnp.repeat(jnp.exp(steps), shape[axis_at] // parts).reshape((-1,) + (1,) * (len(shape) - 1 - axis_at))
    return level


def routed_block(rng, own, number, rows, count, top, bound, lean):
    ranking = jax.random.permutation(rng, count)
    crowded, ordinary = portions_of(count, rows * top, bound, lean, True), portions_of(count, rows * top, bound, lean, False)
    places = jnp.arange(count)

    def named(sizes, offset_by):
        used = int((sizes > 0).sum())
        fixed = max(1, used // 4)
        moved = fixed + (places - fixed + offset_by * (used - fixed)) % max(1, count - fixed)
        return jnp.zeros((count,), jnp.int32).at[ranking[jnp.where(places < fixed, places, moved)]].set(jnp.asarray(sizes, jnp.int32))

    sizes = jnp.where(number % 4 == 0, named(crowded, number // 4), named(ordinary, number - number // 4 - 1))
    mixed = jax.random.permutation(jax.random.fold_in(own, 3), count)
    giver, sink = mixed[0:count // 2 * 2:2], mixed[1:count // 2 * 2:2]
    slack = jnp.minimum(sizes[giver] - 1, bound - sizes[sink]) // 2
    slack = jnp.where((giver == ranking[0]) | (sink == ranking[0]) | (sizes[sink] == 0), 0, jnp.maximum(slack, 0))
    moved = jax.random.randint(jax.random.fold_in(own, 4), (count // 2,), 0, 1 << 20) % (slack + 1)
    sizes = sizes.at[giver].add(-moved).at[sink].add(moved)
    labels = jnp.searchsorted(jnp.cumsum(sizes), jnp.arange(rows * top), side="right").astype(jnp.int32)
    grid = labels.reshape(top, rows).T
    grid = grid[jax.random.permutation(jax.random.fold_in(own, 1), rows)]
    offset_by = jax.random.randint(jax.random.fold_in(own, 2), (rows, 1), 0, top)
    return jnp.take_along_axis(grid, (jnp.arange(top)[None, :] + offset_by) % top, axis=1)


def portions_of(number_of, total, bound, skew, full):
    portions = [(1 << 20) // math.isqrt(standing ** skew) + 1 for standing in range(1, number_of + 1)]
    largest = bound if full else min(bound, max(-(-total // number_of), total * portions[0] // sum(portions)))
    least = 1 if total - largest >= number_of - 1 else 0
    counts, rest = [largest] + [least] * (number_of - 1), total - largest - least * (number_of - 1)
    while rest > 0:
        free = [i for i in range(1, number_of) if counts[i] < largest] or [i for i in range(1, number_of) if counts[i] < bound]
        whole, budget = sum([portions[i] for i in free]), rest
        for i in free:
            more = min(bound - counts[i], max(1, budget * portions[i] // whole), rest)
            counts[i] = counts[i] + more
            rest = rest - more
    return np.array(counts)


def normal_values(key, dims, spread, reach, cuts=(), held_as=jnp.bfloat16):
    array = spread * jax.random.normal(key, dims, jnp.float32)
    if cuts:
        array = array * level_of(key, dims, cuts, -0.22, 0.18)
    return jnp.clip(array, -reach, reach).astype(held_as)


def setup_inputs(seed: int = 0) -> dict:
    splits = jax.random.split(jax.random.key(seed), 22)
    tokens = normal_values(splits[0], (SEQS, D), 1.0, 6.0, ((0, 16),))
    norm_gain = jnp.clip(1.0 + 0.18 * jax.random.normal(splits[1], (D,), jnp.float32), 0.1, 1.9)
    w_query = normal_values(splits[2], (D, HEADS * HEAD_DIM), D ** -0.5, 0.125, ((1, 16),))
    w_key = normal_values(splits[3], (D, HEADS * HEAD_DIM), D ** -0.5, 0.125, ((1, 16),))
    w_value = normal_values(splits[4], (D, HEADS * HEAD_DIM), D ** -0.5, 0.125, ((1, 16),))
    query_gain = jnp.clip(1.0 + 0.18 * jax.random.normal(splits[5], (HEAD_DIM,), jnp.float32), 0.1, 1.9)
    key_gain = jnp.clip(1.0 + 0.18 * jax.random.normal(splits[6], (HEAD_DIM,), jnp.float32), 0.1, 1.9)
    score_bias = draw_score_bias(jax.random.fold_in(splits[21], 71), 0)
    key_cache = normal_values(splits[8], (SEQS, CACHE_LEN, HEADS * HEAD_DIM), 1.0, 6.0, ((0, 16), (2, 16)))
    value_cache = normal_values(splits[9], (SEQS, CACHE_LEN, HEADS * HEAD_DIM), 1.0, 6.0, ((0, 16), (2, 16)))
    lengths = with_ends(jax.random.randint(splits[10], (SEQS,), CACHE_LEN // 8, CACHE_LEN + 1), jax.random.fold_in(splits[10], 1), CACHE_LEN // 8, CACHE_LEN).astype(jnp.int32)
    w_out = normal_values(splits[11], (HEADS * HEAD_DIM, D), (HEADS * HEAD_DIM) ** -0.5, 0.125, ((0, 16),))
    post_gain = jnp.clip(1.0 + 0.18 * jax.random.normal(splits[12], (D,), jnp.float32), 0.1, 1.9)
    routes_keys = jax.random.split(jax.random.fold_in(splits[13], 1), SEQS // SEQ_DEV)
    routes_turns = jax.random.permutation(jax.random.fold_in(splits[13], 3), SEQS // SEQ_DEV)
    routes = jax.vmap(lambda own, number: routed_block(jax.random.fold_in(splits[13], 2), own, number, SEQ_DEV, EXPERTS, TOPK, CAP, 2))(routes_keys, routes_turns).reshape((SEQS, TOPK))
    route_weight = jnp.clip(jnp.exp(math.log(2.0) - 2.0794415 * jax.random.uniform(splits[14], (SEQS, TOPK), jnp.float32) ** level_of(splits[14], (SEQS, TOPK), ((0, 16),), -0.2, 0.2)), 0.25, 2.0)
    expert_gate = normal_values(splits[15], (EXPERTS * 4, D, EXPERT_DIM // 4), D ** -0.5, 0.125, ((0, 256),))
    expert_up = normal_values(splits[16], (EXPERTS * 4, D, EXPERT_DIM // 4), D ** -0.5, 0.125, ((0, 256),))
    expert_down = normal_values(splits[17], (EXPERTS * 4, EXPERT_DIM // 4, D), EXPERT_DIM ** -0.5, 0.25, ((0, 256),))
    shared_gate = normal_values(splits[18], (D, SHARED_DIM), D ** -0.5, 0.125, ((1, 16),))
    shared_up = normal_values(splits[19], (D, SHARED_DIM), D ** -0.5, 0.125, ((1, 16),))
    shared_down = normal_values(splits[20], (SHARED_DIM, D), SHARED_DIM ** -0.5, 0.25, ((0, 16),))
    return dict(tokens=tokens, norm_gain=norm_gain, w_query=w_query, w_key=w_key, w_value=w_value, query_gain=query_gain, key_gain=key_gain, score_bias=score_bias, key_cache=key_cache, value_cache=value_cache, lengths=lengths, w_out=w_out, post_gain=post_gain, routes=routes, route_weight=route_weight, expert_gate=expert_gate, expert_up=expert_up, expert_down=expert_down, shared_gate=shared_gate, shared_up=shared_up, shared_down=shared_down)


EPS = 1e-06

def rms_scale(values, gain_vec):
    mean_sq = lax.optimization_barrier(jnp.mean(values * values, axis=-1, keepdims=True))
    return values * lax.rsqrt(mean_sq + EPS) * gain_vec

def reference(tokens, norm_gain, w_query, w_key, w_value, query_gain, key_gain, score_bias, key_cache, value_cache, lengths, w_out, post_gain, routes, route_weight, expert_gate, expert_up, expert_down, shared_gate, shared_up, shared_down):
    seq_count = tokens.shape[0]
    normed = rms_scale(tokens.astype(jnp.float32), norm_gain).astype(jnp.bfloat16)
    queries = jnp.dot(normed, w_query, preferred_element_type=jnp.float32).reshape(seq_count, HEADS, HEAD_DIM)
    queries = rms_scale(queries, query_gain).astype(jnp.bfloat16)
    key_proj = jnp.dot(normed, w_key, preferred_element_type=jnp.float32).reshape(seq_count, HEADS, HEAD_DIM)
    new_keys = rms_scale(key_proj, key_gain).astype(jnp.bfloat16).reshape(seq_count, HEADS * HEAD_DIM)
    new_values = jnp.dot(normed, w_value, preferred_element_type=jnp.float32).astype(jnp.bfloat16)
    positions = jnp.arange(CACHE_LEN, dtype=jnp.int32)

    def attend(item_parts):
        query_row, key_rows, value_rows, length = item_parts
        key_full = key_rows.astype(jnp.float32).reshape(CACHE_LEN, HEADS, HEAD_DIM)
        value_full = value_rows.astype(jnp.float32).reshape(CACHE_LEN, HEADS, HEAD_DIM)
        logits = jnp.einsum('hd,lhd->hl', query_row.astype(jnp.float32), key_full) * HEAD_DIM ** (-0.5)
        logits = logits + score_bias[:, None]
        visible = (positions < length)[None, :]
        log_beta = jax.nn.log_sigmoid(logits)
        log_keep = jnp.where(visible, jax.nn.log_sigmoid(-logits), 0.0)
        later_sum = lax.cumsum(log_keep, axis=1, reverse=True) - log_keep
        weights = jnp.where(visible, jnp.exp(log_beta + later_sum), 0.0).astype(jnp.bfloat16)
        result = jnp.einsum('hl,lhd->hd', weights.astype(jnp.float32), value_full)
        return result.astype(jnp.bfloat16).reshape(HEADS * HEAD_DIM)
    attended = lax.map(attend, (queries, key_cache, value_cache, lengths))
    attn = jnp.dot(attended, w_out, preferred_element_type=jnp.float32)
    hstate = (tokens.astype(jnp.float32) + attn).astype(jnp.bfloat16)
    h_normed = rms_scale(hstate.astype(jnp.float32), post_gain).astype(jnp.bfloat16)
    expert_ids = jnp.arange(EXPERTS, dtype=jnp.int32)
    chosen = (routes[:, :, None] == expert_ids[None, None, :]).astype(jnp.float32)
    coefs = lax.optimization_barrier(jnp.sum(chosen * route_weight[:, :, None], axis=1))
    quarter = EXPERT_DIM // 4
    gate_full = jnp.transpose(expert_gate.reshape(EXPERTS, 4, D, quarter), (0, 2, 1, 3)).reshape(EXPERTS, D, EXPERT_DIM)
    up_full = jnp.transpose(expert_up.reshape(EXPERTS, 4, D, quarter), (0, 2, 1, 3)).reshape(EXPERTS, D, EXPERT_DIM)
    down_full = expert_down.reshape(EXPERTS, EXPERT_DIM, D)

    def one_expert(running, item_parts):
        gate_w, up_w, down_w, column = item_parts
        gate_pre = jnp.dot(h_normed, gate_w, preferred_element_type=jnp.float32)
        up_pre = jnp.dot(h_normed, up_w, preferred_element_type=jnp.float32)
        hidden = (jax.nn.silu(gate_pre) * up_pre).astype(jnp.bfloat16)
        result = jnp.dot(hidden, down_w, preferred_element_type=jnp.float32)
        return (running + column[:, None] * result, None)
    routed, _ = lax.scan(one_expert, jnp.zeros((seq_count, D), jnp.float32), (gate_full, up_full, down_full, coefs.T))
    shared_hidden = (jax.nn.silu(jnp.dot(h_normed, shared_gate, preferred_element_type=jnp.float32)) * jnp.dot(h_normed, shared_up, preferred_element_type=jnp.float32)).astype(jnp.bfloat16)
    shared = jnp.dot(shared_hidden, shared_down, preferred_element_type=jnp.float32)
    mixed = (hstate.astype(jnp.float32) + shared + routed).astype(jnp.bfloat16)
    return (mixed, new_keys, new_values)
```

```python
import jax
import jax.numpy as jnp
from jax import lax
from jax.experimental import pallas as pl
from jax.experimental.pallas import tpu as pltpu
from jax.sharding import Mesh, PartitionSpec as P

EPS = 1e-06
BF16 = jnp.bfloat16
F32 = jnp.float32
LANES = 128
EP, TA, TB = 16, 4, 4
ROWS = 16
SLOTS = 4
GROUP = 4
BLOCKS = 16
MIB = 1024 * 1024


def rms_rows(values, gain):
    mean_sq = jnp.mean(values * values, axis=-1, keepdims=True)
    return values * lax.rsqrt(mean_sq + EPS) * gain


def dot(x, w):
    return jnp.dot(x, w, preferred_element_type=F32)


def dot_nt(x, w):
    return lax.dot_general(x, w, (((1,), (1,)), ((), ())), preferred_element_type=F32)


def vmem():
    return pl.BlockSpec(memory_space=pltpu.VMEM)


def smem():
    return pl.BlockSpec(memory_space=pltpu.SMEM)


def hbm():
    return pl.BlockSpec(memory_space=pltpu.HBM)


def route_tables(routes, weights, a, pick_ref, coef_hi_ref, coef_lo_ref):
    experts = EP * TA
    expert_ids = lax.broadcasted_iota(jnp.int32, (experts, ROWS), 0)
    member = jnp.zeros((experts, ROWS), F32)
    weight_of = jnp.zeros((experts, ROWS), F32)
    for k in range(routes.shape[0]):
        hit = routes[k : k + 1, :] == expert_ids
        member = member + jnp.where(hit, 1.0, 0.0)
        weight_of = weight_of + jnp.where(hit, weights[k : k + 1, :], 0.0)
    row_in = lax.broadcasted_iota(jnp.int32, (ROWS, ROWS), 0)
    row_out = lax.broadcasted_iota(jnp.int32, (ROWS, ROWS), 1)
    rank = dot(member.astype(BF16), (row_in < row_out).astype(F32).astype(BF16))
    slot_of = (member * (rank + 1.0)).astype(BF16)

    count = EP * TB * TA * SLOTS
    wide_in = lax.broadcasted_iota(jnp.int32, (ROWS, 64), 0)
    wide_out = lax.broadcasted_iota(jnp.int32, (ROWS, 64), 1)
    widen = (wide_out % ROWS == wide_in).astype(F32).astype(BF16)
    row = lax.broadcasted_iota(jnp.int32, (count, 64), 0)
    lane = lax.broadcasted_iota(jnp.int32, (count, 64), 1)
    owner = (lane == (row // 64) * TA + a).astype(F32).astype(BF16)
    found = dot(owner, dot(slot_of, widen).astype(BF16))
    slot = row % SLOTS
    same_block = (row // SLOTS) % TA == lane // ROWS
    routed = found == (slot + 1).astype(F32)
    shared = lane % ROWS == row // 64
    chosen = jnp.where(slot == SLOTS - 1, shared.astype(F32), routed.astype(F32))
    pick_ref[...] = jnp.where(same_block, chosen, 0.0).astype(BF16)

    turn = (row_in == row_out).astype(F32).astype(BF16)
    spread_row = lax.broadcasted_iota(jnp.int32, (experts, count), 0)
    spread_lane = lax.broadcasted_iota(jnp.int32, (experts, count), 1)
    spread = (spread_row == spread_lane // 16).astype(F32).astype(BF16)
    hi = weight_of.astype(BF16)
    lo = (weight_of - hi.astype(F32)).astype(BF16)
    turned = dot_nt(turn, jnp.concatenate([slot_of, hi, lo], axis=0)).astype(BF16)
    by_col = dot(
        jnp.concatenate([turned[:, n * experts : (n + 1) * experts] for n in range(3)], axis=0),
        spread,
    )
    col = lax.broadcasted_iota(jnp.int32, (ROWS, count), 1)
    token = lax.broadcasted_iota(jnp.int32, (ROWS, count), 0)
    col_slot = col % SLOTS
    held = by_col[:ROWS] == (col_slot + 1).astype(F32)
    is_shared = col_slot == SLOTS - 1
    own_shared = (token == col // 64).astype(F32)
    coef_hi_ref[...] = jnp.where(
        is_shared, own_shared, jnp.where(held, by_col[ROWS : 2 * ROWS], 0.0)
    ).astype(BF16)
    coef_lo_ref[...] = jnp.where(is_shared | ~held, 0.0, by_col[2 * ROWS :]).astype(BF16)


def attention_kernel(
    place_ref,
    bias_hbm,
    lengths_hbm,
    norm_gain_hbm,
    query_gain_hbm,
    key_gain_hbm,
    routes_hbm,
    route_weight_hbm,
    tokens_hbm,
    wq_hbm,
    wk_hbm,
    wv_hbm,
    key_hbm,
    value_hbm,
    wout_hbm,
    out_ref,
    new_keys_hbm,
    new_values_hbm,
    tok_slice_ref,
    pick_ref,
    coef_hi_ref,
    coef_lo_ref,
    bias_buf,
    lengths_buf,
    norm_gain_buf,
    query_gain_buf,
    key_gain_buf,
    routes_buf,
    route_weight_buf,
    tokens_buf,
    wq_buf,
    wk_buf,
    wv_buf,
    key_buf,
    value_buf,
    wout_buf,
    q_buf,
    z_buf,
    w_buf,
    att_buf,
    length_rows,
    new_keys_buf,
    new_values_buf,
    small_sem,
    sem,
    key_sem,
    value_sem,
    out_sem,
):
    a, b = place_ref[0], place_ref[1]
    small = [
        pltpu.make_async_copy(src, dst, small_sem.at[n])
        for n, (src, dst) in enumerate(
            (
                (routes_hbm, routes_buf),
                (route_weight_hbm, route_weight_buf),
                (norm_gain_hbm, norm_gain_buf),
                (query_gain_hbm, query_gain_buf),
                (key_gain_hbm, key_gain_buf),
                (lengths_hbm, lengths_buf),
                (bias_hbm, bias_buf),
            )
        )
    ]
    large = [
        pltpu.make_async_copy(src, dst, sem.at[n])
        for n, (src, dst) in enumerate(
            (
                (tokens_hbm, tokens_buf),
                (wq_hbm, wq_buf),
                (wk_hbm, wk_buf),
                (wv_hbm, wv_buf),
                (wout_hbm, wout_buf),
            )
        )
    ]
    groups = ROWS // GROUP
    key_copies, value_copies = (
        [
            pltpu.make_async_copy(
                src.at[pl.ds(g * GROUP, GROUP)], dst.at[pl.ds(g * GROUP, GROUP)], sems.at[g]
            )
            for g in range(groups)
        ]
        for src, dst, sems in (
            (key_hbm, key_buf, key_sem),
            (value_hbm, value_buf, value_sem),
        )
    )
    for copy in small + large[:2] + key_copies + large[2:4] + value_copies + large[4:]:
        copy.start()

    cache_len = key_buf.shape[1]
    head_size = key_buf.shape[2]
    for copy in small:
        copy.wait()
    route_tables(
        routes_buf[...], route_weight_buf[...], a, pick_ref, coef_hi_ref, coef_lo_ref
    )
    for s in range(ROWS):
        length_rows[s : s + 1, :] = jnp.full((1, LANES), lengths_buf[s], jnp.int32)
    for copy in large[:2]:
        copy.wait()
    normed = rms_rows(tokens_buf[...].astype(F32), norm_gain_buf[...]).astype(BF16)
    q_buf[...] = (
        rms_rows(dot(normed, wq_buf[...]), query_gain_buf[...]).astype(BF16).astype(F32)
    )
    for j in range(TA):
        cols = pl.ds(pl.multiple_of((j * TB + b) * LANES, LANES), LANES)
        tok_slice_ref[j * ROWS : (j + 1) * ROWS, :] = tokens_buf[:, cols].astype(F32)

    for g in range(groups):
        key_copies[g].wait()
        for s in range(g * GROUP, (g + 1) * GROUP):
            z_buf[s : s + 1, :] = dot_nt(q_buf[s : s + 1, :].astype(BF16), key_buf[s])

    for copy in large[2:4]:
        copy.wait()
    new_keys_buf[...] = rms_rows(dot(normed, wk_buf[...]), key_gain_buf[...]).astype(BF16)
    new_values_buf[...] = dot(normed, wv_buf[...]).astype(BF16)
    out_copies = [
        pltpu.make_async_copy(new_keys_buf, new_keys_hbm, out_sem.at[0]),
        pltpu.make_async_copy(new_values_buf, new_values_hbm, out_sem.at[1]),
    ]

    chunks = cache_len // LANES
    after = lax.broadcasted_iota(jnp.int32, (3 * LANES, LANES), 0) % LANES
    upto = lax.broadcasted_iota(jnp.int32, (3 * LANES, LANES), 1)
    later = (after > upto).astype(F32).astype(BF16)
    chunk_lane = lax.broadcasted_iota(jnp.int32, (ROWS, LANES), 1)
    logits = z_buf[...] * head_size ** (-0.5) + bias_buf[0]
    soft = jnp.log1p(jnp.exp(-jnp.abs(logits)))
    log_beta = jnp.minimum(logits, 0.0) - soft
    log_not = jnp.minimum(-logits, 0.0) - soft
    visible = [chunk_lane + c * LANES < length_rows[...] for c in range(chunks)]
    stacked = jnp.concatenate(
        [
            jnp.where(visible[c], log_not[:, c * LANES : (c + 1) * LANES], 0.0)
            for c in range(chunks)
        ],
        axis=0,
    )
    first = stacked.astype(BF16)
    rest = stacked - first.astype(F32)
    second = rest.astype(BF16)
    third = (rest - second.astype(F32)).astype(BF16)
    inner = dot(jnp.concatenate([first, second, third], axis=1), later)
    totals = jnp.sum(stacked, axis=1, keepdims=True)
    carry = jnp.zeros((ROWS, 1), F32)
    for c in reversed(range(chunks)):
        cols = slice(c * LANES, (c + 1) * LANES)
        later_sum = inner[c * ROWS : (c + 1) * ROWS, :] + carry
        w_buf[:, cols] = jnp.where(visible[c], jnp.exp(log_beta[:, cols] + later_sum), 0.0)
        carry = carry + totals[c * ROWS : (c + 1) * ROWS, :]

    for copy in out_copies:
        copy.start()
    for g in range(groups):
        value_copies[g].wait()
        for s in range(g * GROUP, (g + 1) * GROUP):
            att_buf[s : s + 1, :] = dot(w_buf[s : s + 1, :].astype(BF16), value_buf[s])
    large[4].wait()
    attn = dot(att_buf[...].astype(BF16), wout_buf[...]).astype(BF16)
    for t in range(BLOCKS):
        block = attn[:, t * LANES : (t + 1) * LANES]
        j, quarter = t // TB, t % TB
        for n in range(TA):
            start = (n * TB + quarter) * 64 + j * ROWS
            out_ref[start : start + ROWS, :] = block
    for copy in out_copies:
        copy.wait()


def attention(
    place,
    bias,
    lengths,
    norm_gain,
    query_gain,
    key_gain,
    routes,
    route_weight,
    tokens,
    wq,
    wk,
    wv,
    keys,
    values,
    wout,
):
    rows, cache_len, head_size = keys.shape
    width = tokens.shape[1]
    shape = jax.ShapeDtypeStruct
    return pl.pallas_call(
        attention_kernel,
        name="attention",
        out_shape=(
            shape((1024, LANES), BF16),
            shape((rows, head_size), BF16),
            shape((rows, head_size), BF16),
            shape((64, LANES), F32),
            shape((1024, 64), BF16),
            shape((rows, 1024), BF16),
            shape((rows, 1024), BF16),
        ),
        in_specs=[smem()] + [hbm()] * 14,
        out_specs=(vmem(), hbm(), hbm(), vmem(), vmem(), vmem(), vmem()),
        scratch_shapes=[
            pltpu.SMEM(bias.shape, F32),
            pltpu.SMEM(lengths.shape, jnp.int32),
            pltpu.VMEM(norm_gain.shape, F32),
            pltpu.VMEM(query_gain.shape, F32),
            pltpu.VMEM(key_gain.shape, F32),
            pltpu.VMEM(routes.shape, jnp.int32),
            pltpu.VMEM(route_weight.shape, F32),
            pltpu.VMEM((rows, width), BF16),
            pltpu.VMEM((width, head_size), BF16),
            pltpu.VMEM((width, head_size), BF16),
            pltpu.VMEM((width, head_size), BF16),
            pltpu.VMEM((rows, cache_len, head_size), BF16),
            pltpu.VMEM((rows, cache_len, head_size), BF16),
            pltpu.VMEM((head_size, width), BF16),
            pltpu.VMEM((rows, head_size), F32),
            pltpu.VMEM((rows, cache_len), F32),
            pltpu.VMEM((rows, cache_len), F32),
            pltpu.VMEM((rows, head_size), F32),
            pltpu.VMEM((rows, LANES), jnp.int32),
            pltpu.VMEM((rows, head_size), BF16),
            pltpu.VMEM((rows, head_size), BF16),
            pltpu.SemaphoreType.DMA((7,)),
            pltpu.SemaphoreType.DMA((5,)),
            pltpu.SemaphoreType.DMA((rows // GROUP,)),
            pltpu.SemaphoreType.DMA((rows // GROUP,)),
            pltpu.SemaphoreType.DMA((2,)),
        ],
        cost_estimate=pl.CostEstimate(
            flops=2_000_000_000, bytes_accessed=10 * MIB, transcendentals=0
        ),
        compiler_params=pltpu.CompilerParams(vmem_limit_bytes=56 * MIB),
    )(
        place,
        bias,
        lengths,
        norm_gain,
        query_gain,
        key_gain,
        routes,
        route_weight,
        tokens,
        wq,
        wk,
        wv,
        keys,
        values,
        wout,
    )


def dispatch_kernel(place_ref, arrived_ref, tok_slice_ref, pick_ref, out_ref, own_ref, h_buf):
    total = tok_slice_ref[...]
    parts = [arrived_ref[n * 64 : (n + 1) * 64, :].astype(F32) for n in range(TA * TB)]
    while len(parts) > 1:
        parts = [parts[n] + parts[n + 1] for n in range(0, len(parts), 2)]
    h = (total + parts[0]).astype(BF16)
    h_buf[...] = h.astype(F32)
    out_ref[...] = dot(pick_ref[...], h).astype(BF16)
    own_ref[...] = h_buf[pl.ds(pl.multiple_of(place_ref[0] * ROWS, ROWS), ROWS), :]


def dispatch(place, arrived, tok_slice, pick):
    shape = jax.ShapeDtypeStruct
    return pl.pallas_call(
        dispatch_kernel,
        name="dispatch",
        out_shape=(shape((1024, LANES), BF16), shape((ROWS, LANES), F32)),
        in_specs=[smem()] + [vmem()] * 3,
        out_specs=(vmem(),) * 2,
        scratch_shapes=[pltpu.VMEM((64, LANES), F32)],
        cost_estimate=pl.CostEstimate(
            flops=500_000_000, bytes_accessed=MIB, transcendentals=0
        ),
        compiler_params=pltpu.CompilerParams(vmem_limit_bytes=4 * MIB),
    )(place, arrived, tok_slice, pick)


def expert_kernel(
    arrived_ref,
    post_gain_ref,
    gate_ref,
    up_ref,
    down_ref,
    shared_gate_ref,
    shared_up_ref,
    shared_down_ref,
    out_ref,
    rows_buf,
    x_buf,
    send_buf,
):
    rows_buf[...] = arrived_ref[...].astype(F32)
    for t in range(BLOCKS):
        j, b = t // TB, t % TB
        for s in range(SLOTS):
            x_buf[s * ROWS : (s + 1) * ROWS, t * LANES : (t + 1) * LANES] = rows_buf[
                pl.ds(b * 16 + j * SLOTS + s, EP, stride=64), :
            ]
    h_normed = rms_rows(x_buf[...], post_gain_ref[...]).astype(BF16)
    routed_rows, shared_rows = h_normed[:48], h_normed[48:]
    gate = dot(routed_rows, gate_ref[...])
    up = dot(routed_rows, up_ref[...])
    hidden = (gate * jax.nn.sigmoid(gate) * up).astype(BF16)
    s_gate = dot_nt(shared_rows, shared_gate_ref[...])
    s_up = dot_nt(shared_rows, shared_up_ref[...])
    s_hidden = (s_gate * jax.nn.sigmoid(s_gate) * s_up).astype(BF16)
    routed = dot(hidden, down_ref[...])
    shared = dot(s_hidden, shared_down_ref[...])
    for t in range(BLOCKS):
        cols = slice(t * LANES, (t + 1) * LANES)
        for s in range(SLOTS):
            part = routed[s * ROWS : (s + 1) * ROWS, cols] if s < SLOTS - 1 else shared[:, cols]
            send_buf[pl.ds(t * SLOTS + s, EP, stride=64), :] = part
    out_ref[...] = send_buf[...].astype(BF16)


def run_experts(arrived, post_gain, gate, up, down, s_gate, s_up, s_down):
    return pl.pallas_call(
        expert_kernel,
        name="experts",
        out_shape=jax.ShapeDtypeStruct((1024, LANES), BF16),
        in_specs=[vmem()] * 8,
        out_specs=vmem(),
        scratch_shapes=[
            pltpu.VMEM((1024, LANES), F32),
            pltpu.VMEM((64, BLOCKS * LANES), F32),
            pltpu.VMEM((1024, LANES), F32),
        ],
        cost_estimate=pl.CostEstimate(
            flops=1_000_000_000, bytes_accessed=3 * MIB, transcendentals=0
        ),
        compiler_params=pltpu.CompilerParams(vmem_limit_bytes=12 * MIB),
    )(arrived, post_gain, gate, up, down, s_gate, s_up, s_down)


def combine_kernel(arrived_ref, coef_hi_ref, coef_lo_ref, own_ref, out_ref):
    arrived = arrived_ref[...]
    both = dot(jnp.concatenate([coef_hi_ref[...], coef_lo_ref[...]], axis=0), arrived)
    out_ref[...] = (own_ref[...] + (both[:ROWS] + both[ROWS:])).astype(BF16)


def combine(arrived, coef_hi, coef_lo, own):
    return pl.pallas_call(
        combine_kernel,
        name="combine",
        out_shape=jax.ShapeDtypeStruct((ROWS, LANES), BF16),
        in_specs=[vmem()] * 4,
        out_specs=vmem(),
        cost_estimate=pl.CostEstimate(
            flops=100_000_000, bytes_accessed=MIB, transcendentals=0
        ),
        compiler_params=pltpu.CompilerParams(vmem_limit_bytes=4 * MIB),
    )(arrived, coef_hi, coef_lo, own)


def exchange(x, axes, parts):
    pieces = x.reshape(parts, -1, LANES)
    arrived = lax.all_to_all(pieces, axes, split_axis=0, concat_axis=0, tiled=True)
    return arrived.reshape(x.shape)


def local(
    tokens,
    norm_gain,
    w_query,
    w_key,
    w_value,
    query_gain,
    key_gain,
    score_bias,
    key_cache,
    value_cache,
    lengths,
    w_out,
    post_gain,
    routes,
    route_weight,
    expert_gate,
    expert_up,
    expert_down,
    shared_gate,
    shared_up,
    shared_down,
):
    place = jnp.stack([lax.axis_index("ta"), lax.axis_index("tb")]).astype(jnp.int32)
    partial_rows, new_keys, new_values, tok_slice, pick, coef_hi, coef_lo = attention(
        place,
        score_bias,
        lengths,
        norm_gain[None, :],
        query_gain[None, :],
        key_gain[None, :],
        routes.T,
        route_weight.T,
        tokens,
        w_query,
        w_key,
        w_value,
        key_cache,
        value_cache,
        w_out,
    )
    arrived = exchange(partial_rows, ("ta", "tb"), TA * TB)
    outgoing, own = dispatch(place, arrived, tok_slice, pick)
    received = exchange(outgoing, ("ep", "tb"), EP * TB)
    parts = run_experts(
        received,
        post_gain[None, :],
        expert_gate[0],
        expert_up[0],
        expert_down[0],
        shared_gate.T,
        shared_up.T,
        shared_down,
    )
    returned = exchange(parts, ("ep", "ta", "tb"), EP * TA * TB)
    mixed = combine(returned, coef_hi, coef_lo, own)
    return (mixed, new_keys, new_values)


def solution(mesh):
    cut = Mesh(mesh.devices.reshape(EP, TA, TB), ("ep", "ta", "tb"))
    tp = ("ta", "tb")
    placed = (
        P("ep", None),
        P(),
        P(None, tp),
        P(None, tp),
        P(None, tp),
        P(),
        P(),
        P(tp),
        P("ep", None, tp),
        P("ep", None, tp),
        P("ep"),
        P(tp, None),
        P(),
        P("ep", None),
        P("ep", None),
        P(("ep", "ta", "tb"), None, None),
        P(("ep", "ta", "tb"), None, None),
        P(("ep", "ta", "tb"), None, None),
        P(None, tp),
        P(None, tp),
        P(tp, None),
    )
    return jax.shard_map(
        local,
        mesh=cut,
        in_specs=placed,
        out_specs=(P("ep", tp),) * 3,
        check_vma=False,
    )
```

```python
import jax
import jax.numpy as jnp
from jax import lax
from jax.experimental import pallas as pl
from jax.experimental.pallas import tpu as pltpu
from jax.sharding import Mesh, PartitionSpec as P

EPS = 1e-06
BF16 = jnp.bfloat16
F32 = jnp.float32
LANES = 128
EP, TA, TB = 16, 4, 4
ROWS = 16
SLOTS = 4
GROUP = 4
HEAD_ROWS = 256
TILE = 16
BLOCKS = 16
MIB = 1024 * 1024


def rms_rows(values, gain):
    mean_sq = jnp.mean(values * values, axis=-1, keepdims=True)
    return values * lax.rsqrt(mean_sq + EPS) * gain


def dot(x, w):
    return jnp.dot(x, w, preferred_element_type=F32)


def dot_nt(x, w):
    return lax.dot_general(x, w, (((1,), (1,)), ((), ())), preferred_element_type=F32)


def vmem():
    return pl.BlockSpec(memory_space=pltpu.VMEM)


def hbm():
    return pl.BlockSpec(memory_space=pltpu.HBM)


def route_tables(routes, weights, a, pick_ref, coef_hi_ref, coef_lo_ref):
    experts = EP * TA
    expert_ids = lax.broadcasted_iota(jnp.int32, (experts, ROWS), 0)
    member = jnp.zeros((experts, ROWS), F32)
    weight_of = jnp.zeros((experts, ROWS), F32)
    for k in range(routes.shape[0]):
        hit = routes[k : k + 1, :] == expert_ids
        member = member + jnp.where(hit, 1.0, 0.0)
        weight_of = weight_of + jnp.where(hit, weights[k : k + 1, :], 0.0)
    row_in = lax.broadcasted_iota(jnp.int32, (ROWS, ROWS), 0)
    row_out = lax.broadcasted_iota(jnp.int32, (ROWS, ROWS), 1)
    rank = dot(member.astype(BF16), (row_in < row_out).astype(F32).astype(BF16))
    slot_of = (member * (rank + 1.0)).astype(BF16)

    count = EP * TB * TA * SLOTS
    wide_in = lax.broadcasted_iota(jnp.int32, (ROWS, 64), 0)
    wide_out = lax.broadcasted_iota(jnp.int32, (ROWS, 64), 1)
    widen = (wide_out % ROWS == wide_in).astype(F32).astype(BF16)
    row = lax.broadcasted_iota(jnp.int32, (count, 64), 0)
    lane = lax.broadcasted_iota(jnp.int32, (count, 64), 1)
    owner = (lane == (row // 64) * TA + a).astype(F32).astype(BF16)
    found = dot(owner, dot(slot_of, widen).astype(BF16))
    slot = row % SLOTS
    same_block = (row // SLOTS) % TA == lane // ROWS
    routed = found == (slot + 1).astype(F32)
    shared = lane % ROWS == row // 64
    chosen = jnp.where(slot == SLOTS - 1, shared.astype(F32), routed.astype(F32))
    pick_ref[...] = jnp.where(same_block, chosen, 0.0).astype(BF16)

    turn = (row_in == row_out).astype(F32).astype(BF16)
    spread_row = lax.broadcasted_iota(jnp.int32, (experts, count), 0)
    spread_lane = lax.broadcasted_iota(jnp.int32, (experts, count), 1)
    spread = (spread_row == spread_lane // 16).astype(F32).astype(BF16)
    hi = weight_of.astype(BF16)
    lo = (weight_of - hi.astype(F32)).astype(BF16)
    turned = dot_nt(turn, jnp.concatenate([slot_of, hi, lo], axis=0)).astype(BF16)
    by_col = dot(
        jnp.concatenate([turned[:, n * experts : (n + 1) * experts] for n in range(3)], axis=0),
        spread,
    )
    col = lax.broadcasted_iota(jnp.int32, (ROWS, count), 1)
    token = lax.broadcasted_iota(jnp.int32, (ROWS, count), 0)
    col_slot = col % SLOTS
    held = by_col[:ROWS] == (col_slot + 1).astype(F32)
    is_shared = col_slot == SLOTS - 1
    own_shared = (token == col // 64).astype(F32)
    coef_hi_ref[...] = jnp.where(
        is_shared, own_shared, jnp.where(held, by_col[ROWS : 2 * ROWS], 0.0)
    ).astype(BF16)
    coef_lo_ref[...] = jnp.where(is_shared | ~held, 0.0, by_col[2 * ROWS :]).astype(BF16)


def attention_kernel(
    bias_hbm,
    lengths_hbm,
    norm_gain_hbm,
    query_gain_hbm,
    key_gain_hbm,
    routes_hbm,
    route_weight_hbm,
    tokens_hbm,
    wq_hbm,
    wk_hbm,
    wv_hbm,
    key_hbm,
    value_hbm,
    wout_hbm,
    out_ref,
    new_keys_hbm,
    new_values_hbm,
    tok_slice_ref,
    pick_ref,
    coef_hi_ref,
    coef_lo_ref,
    bias_buf,
    lengths_buf,
    norm_gain_buf,
    query_gain_buf,
    key_gain_buf,
    routes_buf,
    route_weight_buf,
    tokens_buf,
    wq_buf,
    wk_buf,
    wv_buf,
    key_buf,
    value_buf,
    wout_buf,
    q_buf,
    z_buf,
    w_buf,
    att_buf,
    length_rows,
    new_keys_buf,
    new_values_buf,
    small_sem,
    sem,
    key_sem,
    value_sem,
    out_sem,
):
    a, b = lax.axis_index("ta"), lax.axis_index("tb")
    small = [
        pltpu.make_async_copy(src, dst, small_sem.at[n])
        for n, (src, dst) in enumerate(
            (
                (lengths_hbm, lengths_buf),
                (bias_hbm, bias_buf),
                (routes_hbm, routes_buf),
                (route_weight_hbm, route_weight_buf),
                (norm_gain_hbm, norm_gain_buf),
                (query_gain_hbm, query_gain_buf),
                (key_gain_hbm, key_gain_buf),
            )
        )
    ]
    large = [
        pltpu.make_async_copy(src, dst, sem.at[n])
        for n, (src, dst) in enumerate(
            (
                (tokens_hbm, tokens_buf),
                (wq_hbm, wq_buf),
                (wk_hbm, wk_buf),
                (wv_hbm, wv_buf),
                (wout_hbm, wout_buf),
            )
        )
    ]
    cache_len = key_buf.shape[1]
    head_size = key_buf.shape[2]
    caches = ((key_hbm, key_buf, key_sem), (value_hbm, value_buf, value_sem))
    head_copies = [
        pltpu.make_async_copy(
            src.at[:, pl.ds(0, HEAD_ROWS)], dst.at[:, pl.ds(0, HEAD_ROWS)], sems.at[ROWS]
        )
        for src, dst, sems in caches
    ]
    for copy in small + large[:2] + head_copies[:1]:
        copy.start()
    value_buf[:, HEAD_ROWS:, :] = jnp.zeros(
        (ROWS, cache_len - HEAD_ROWS, head_size), value_buf.dtype
    )
    small[0].wait()
    small[1].wait()

    def tail_copy(cache, s):
        src, dst, sems = cache
        tiles = jnp.maximum((lengths_buf[s] + TILE - 1) // TILE, HEAD_ROWS // TILE + 1)
        size = pl.multiple_of((tiles - HEAD_ROWS // TILE) * TILE, TILE)
        part = pl.ds(HEAD_ROWS, size)
        return pltpu.make_async_copy(src.at[s, part], dst.at[s, part], sems.at[s])

    key_copies, value_copies = ([tail_copy(cache, s) for s in range(ROWS)] for cache in caches)
    for copy in key_copies + head_copies[1:]:
        copy.start()

    for copy in small[2:]:
        copy.wait()
    route_tables(
        routes_buf[...], route_weight_buf[...], a, pick_ref, coef_hi_ref, coef_lo_ref
    )
    for s in range(ROWS):
        length_rows[s : s + 1, :] = jnp.full((1, LANES), lengths_buf[s], jnp.int32)
    for copy in large[:2]:
        copy.wait()
    normed = rms_rows(tokens_buf[...].astype(F32), norm_gain_buf[...]).astype(BF16)
    q_buf[...] = (
        rms_rows(dot(normed, wq_buf[...]), query_gain_buf[...]).astype(BF16).astype(F32)
    )
    for j in range(TA):
        cols = pl.ds(pl.multiple_of((j * TB + b) * LANES, LANES), LANES)
        tok_slice_ref[j * ROWS : (j + 1) * ROWS, :] = tokens_buf[:, cols].astype(F32)

    head_copies[0].wait()
    for g in range(ROWS // GROUP):
        members = range(g * GROUP, (g + 1) * GROUP)
        for s in members:
            key_copies[s].wait()
        for s in members:
            value_copies[s].start()
        for s in members:
            z_buf[s : s + 1, :] = dot_nt(q_buf[s : s + 1, :].astype(BF16), key_buf[s])

    for copy in large[2:]:
        copy.start()
    for copy in large[2:4]:
        copy.wait()
    new_keys_buf[...] = rms_rows(dot(normed, wk_buf[...]), key_gain_buf[...]).astype(BF16)
    new_values_buf[...] = dot(normed, wv_buf[...]).astype(BF16)
    out_copies = [
        pltpu.make_async_copy(new_keys_buf, new_keys_hbm, out_sem.at[0]),
        pltpu.make_async_copy(new_values_buf, new_values_hbm, out_sem.at[1]),
    ]

    chunks = cache_len // LANES
    after = lax.broadcasted_iota(jnp.int32, (3 * LANES, LANES), 0) % LANES
    upto = lax.broadcasted_iota(jnp.int32, (3 * LANES, LANES), 1)
    later = (after > upto).astype(F32).astype(BF16)
    chunk_lane = lax.broadcasted_iota(jnp.int32, (ROWS, LANES), 1)
    logits = z_buf[...] * head_size ** (-0.5) + bias_buf[0, 0]
    soft = jnp.log1p(jnp.exp(-jnp.abs(logits)))
    log_beta = jnp.minimum(logits, 0.0) - soft
    log_not = jnp.minimum(-logits, 0.0) - soft
    visible = [chunk_lane + c * LANES < length_rows[...] for c in range(chunks)]
    stacked = jnp.concatenate(
        [
            jnp.where(visible[c], log_not[:, c * LANES : (c + 1) * LANES], 0.0)
            for c in range(chunks)
        ],
        axis=0,
    )
    first = stacked.astype(BF16)
    rest = stacked - first.astype(F32)
    second = rest.astype(BF16)
    third = (rest - second.astype(F32)).astype(BF16)
    inner = dot(jnp.concatenate([first, second, third], axis=1), later)
    totals = jnp.sum(stacked, axis=1, keepdims=True)
    carry = jnp.zeros((ROWS, 1), F32)
    for c in reversed(range(chunks)):
        cols = slice(c * LANES, (c + 1) * LANES)
        later_sum = inner[c * ROWS : (c + 1) * ROWS, :] + carry
        w_buf[:, cols] = jnp.where(visible[c], jnp.exp(log_beta[:, cols] + later_sum), 0.0)
        carry = carry + totals[c * ROWS : (c + 1) * ROWS, :]

    for copy in out_copies:
        copy.start()
    head_copies[1].wait()
    for g in range(ROWS // GROUP):
        members = range(g * GROUP, (g + 1) * GROUP)
        for s in members:
            value_copies[s].wait()
        for s in members:
            att_buf[s : s + 1, :] = dot(w_buf[s : s + 1, :].astype(BF16), value_buf[s])
    large[4].wait()
    attn = dot(att_buf[...].astype(BF16), wout_buf[...]).astype(BF16)
    for t in range(BLOCKS):
        block = attn[:, t * LANES : (t + 1) * LANES]
        j, quarter = t // TB, t % TB
        for n in range(TA):
            start = (n * TB + quarter) * 64 + j * ROWS
            out_ref[start : start + ROWS, :] = block
    for copy in out_copies:
        copy.wait()


def attention(
    bias,
    lengths,
    norm_gain,
    query_gain,
    key_gain,
    routes,
    route_weight,
    tokens,
    wq,
    wk,
    wv,
    keys,
    values,
    wout,
):
    rows, cache_len, head_size = keys.shape
    width = tokens.shape[1]
    shape = jax.ShapeDtypeStruct
    return pl.pallas_call(
        attention_kernel,
        name="attention",
        out_shape=(
            shape((1024, LANES), BF16),
            shape((rows, head_size), BF16),
            shape((rows, head_size), BF16),
            shape((64, LANES), F32),
            shape((1024, 64), BF16),
            shape((rows, 1024), BF16),
            shape((rows, 1024), BF16),
        ),
        in_specs=[hbm()] * 14,
        out_specs=(vmem(), hbm(), hbm(), vmem(), vmem(), vmem(), vmem()),
        scratch_shapes=[
            pltpu.SMEM(bias.shape, F32),
            pltpu.SMEM(lengths.shape, jnp.int32),
            pltpu.VMEM(norm_gain.shape, F32),
            pltpu.VMEM(query_gain.shape, F32),
            pltpu.VMEM(key_gain.shape, F32),
            pltpu.VMEM(routes.shape, jnp.int32),
            pltpu.VMEM(route_weight.shape, F32),
            pltpu.VMEM((rows, width), BF16),
            pltpu.VMEM((width, head_size), BF16),
            pltpu.VMEM((width, head_size), BF16),
            pltpu.VMEM((width, head_size), BF16),
            pltpu.VMEM((rows, cache_len, head_size), BF16),
            pltpu.VMEM((rows, cache_len, head_size), BF16),
            pltpu.VMEM((head_size, width), BF16),
            pltpu.VMEM((rows, head_size), F32),
            pltpu.VMEM((rows, cache_len), F32),
            pltpu.VMEM((rows, cache_len), F32),
            pltpu.VMEM((rows, head_size), F32),
            pltpu.VMEM((rows, LANES), jnp.int32),
            pltpu.VMEM((rows, head_size), BF16),
            pltpu.VMEM((rows, head_size), BF16),
            pltpu.SemaphoreType.DMA((7,)),
            pltpu.SemaphoreType.DMA((5,)),
            pltpu.SemaphoreType.DMA((rows + 1,)),
            pltpu.SemaphoreType.DMA((rows + 1,)),
            pltpu.SemaphoreType.DMA((2,)),
        ],
        cost_estimate=pl.CostEstimate(
            flops=2_000_000_000, bytes_accessed=10 * MIB, transcendentals=0
        ),
        compiler_params=pltpu.CompilerParams(vmem_limit_bytes=16 * MIB),
    )(
        bias,
        *(pltpu.with_memory_space_constraint(x, pltpu.HBM) for x in (
        lengths,
        norm_gain,
        query_gain,
        key_gain,
        routes,
        route_weight,
        tokens,
        wq,
        wk,
        wv,
        keys,
        values,
        wout,
        ))
    )


def dispatch_kernel(arrived_ref, tok_slice_ref, pick_ref, out_ref, own_ref, h_buf):
    total = tok_slice_ref[...]
    parts = [arrived_ref[n * 64 : (n + 1) * 64, :].astype(F32) for n in range(TA * TB)]
    while len(parts) > 1:
        parts = [parts[n] + parts[n + 1] for n in range(0, len(parts), 2)]
    h = (total + parts[0]).astype(BF16)
    h_buf[...] = h.astype(F32)
    out_ref[...] = dot(pick_ref[...], h).astype(BF16)
    own_ref[...] = h_buf[pl.ds(pl.multiple_of(lax.axis_index("ta") * ROWS, ROWS), ROWS), :]


def dispatch(arrived, tok_slice, pick):
    shape = jax.ShapeDtypeStruct
    return pl.pallas_call(
        dispatch_kernel,
        name="dispatch",
        out_shape=(shape((1024, LANES), BF16), shape((ROWS, LANES), F32)),
        in_specs=[vmem()] * 3,
        out_specs=(vmem(),) * 2,
        scratch_shapes=[pltpu.VMEM((64, LANES), F32)],
        cost_estimate=pl.CostEstimate(
            flops=500_000_000, bytes_accessed=MIB, transcendentals=0
        ),
        compiler_params=pltpu.CompilerParams(vmem_limit_bytes=4 * MIB),
    )(arrived, tok_slice, pick)


def expert_kernel(
    arrived_ref,
    post_gain_ref,
    gate_ref,
    up_ref,
    down_ref,
    shared_gate_ref,
    shared_up_ref,
    shared_down_ref,
    out_ref,
    rows_buf,
    x_buf,
    send_buf,
):
    rows_buf[...] = arrived_ref[...].astype(F32)
    for t in range(BLOCKS):
        j, b = t // TB, t % TB
        for s in range(SLOTS):
            x_buf[s * ROWS : (s + 1) * ROWS, t * LANES : (t + 1) * LANES] = rows_buf[
                pl.ds(b * 16 + j * SLOTS + s, EP, stride=64), :
            ]
    h_normed = rms_rows(x_buf[...], post_gain_ref[...]).astype(BF16)
    routed_rows, shared_rows = h_normed[:48], h_normed[48:]
    gate = dot(routed_rows, gate_ref[...])
    up = dot(routed_rows, up_ref[...])
    hidden = (gate * jax.nn.sigmoid(gate) * up).astype(BF16)
    s_gate = dot_nt(shared_rows, shared_gate_ref[...])
    s_up = dot_nt(shared_rows, shared_up_ref[...])
    s_hidden = (s_gate * jax.nn.sigmoid(s_gate) * s_up).astype(BF16)
    routed = dot(hidden, down_ref[...])
    shared = dot(s_hidden, shared_down_ref[...])
    for t in range(BLOCKS):
        cols = slice(t * LANES, (t + 1) * LANES)
        for s in range(SLOTS):
            part = routed[s * ROWS : (s + 1) * ROWS, cols] if s < SLOTS - 1 else shared[:, cols]
            send_buf[pl.ds(t * SLOTS + s, EP, stride=64), :] = part
    out_ref[...] = send_buf[...].astype(BF16)


def run_experts(arrived, post_gain, gate, up, down, s_gate, s_up, s_down):
    return pl.pallas_call(
        expert_kernel,
        name="experts",
        out_shape=jax.ShapeDtypeStruct((1024, LANES), BF16),
        in_specs=[vmem()] * 8,
        out_specs=vmem(),
        scratch_shapes=[
            pltpu.VMEM((1024, LANES), F32),
            pltpu.VMEM((64, BLOCKS * LANES), F32),
            pltpu.VMEM((1024, LANES), F32),
        ],
        cost_estimate=pl.CostEstimate(
            flops=1_000_000_000, bytes_accessed=3 * MIB, transcendentals=0
        ),
        compiler_params=pltpu.CompilerParams(vmem_limit_bytes=12 * MIB),
    )(arrived, post_gain, gate, up, down, s_gate, s_up, s_down)


def combine_kernel(arrived_ref, coef_hi_ref, coef_lo_ref, own_ref, out_ref):
    arrived = arrived_ref[...]
    both = dot(jnp.concatenate([coef_hi_ref[...], coef_lo_ref[...]], axis=0), arrived)
    out_ref[...] = (own_ref[...] + (both[:ROWS] + both[ROWS:])).astype(BF16)


def combine(arrived, coef_hi, coef_lo, own):
    return pl.pallas_call(
        combine_kernel,
        name="combine",
        out_shape=jax.ShapeDtypeStruct((ROWS, LANES), BF16),
        in_specs=[vmem()] * 4,
        out_specs=vmem(),
        cost_estimate=pl.CostEstimate(
            flops=100_000_000, bytes_accessed=MIB, transcendentals=0
        ),
        compiler_params=pltpu.CompilerParams(vmem_limit_bytes=4 * MIB),
    )(arrived, coef_hi, coef_lo, own)


def exchange(x, axes, parts):
    pieces = x.reshape(parts, -1, LANES)
    arrived = lax.all_to_all(pieces, axes, split_axis=0, concat_axis=0, tiled=True)
    return arrived.reshape(x.shape)


def local(
    tokens,
    norm_gain,
    w_query,
    w_key,
    w_value,
    query_gain,
    key_gain,
    score_bias,
    key_cache,
    value_cache,
    lengths,
    w_out,
    post_gain,
    routes,
    route_weight,
    expert_gate,
    expert_up,
    expert_down,
    shared_gate,
    shared_up,
    shared_down,
):
    partial_rows, new_keys, new_values, tok_slice, pick, coef_hi, coef_lo = attention(
        score_bias[None, :],
        lengths,
        norm_gain[None, :],
        query_gain[None, :],
        key_gain[None, :],
        routes.T,
        route_weight.T,
        tokens,
        w_query,
        w_key,
        w_value,
        key_cache,
        value_cache,
        w_out,
    )
    later = (post_gain, expert_gate, expert_up, expert_down, shared_gate, shared_up, shared_down)
    partial_rows, *later = lax.optimization_barrier((partial_rows, *later))
    post_gain, expert_gate, expert_up, expert_down, shared_gate, shared_up, shared_down = later
    arrived = exchange(partial_rows, ("ta", "tb"), TA * TB)
    outgoing, own = dispatch(arrived, tok_slice, pick)
    received = exchange(outgoing, ("ep", "tb"), EP * TB)
    parts = run_experts(
        received,
        post_gain[None, :],
        expert_gate[0],
        expert_up[0],
        expert_down[0],
        shared_gate.T,
        shared_up.T,
        shared_down,
    )
    returned = exchange(parts, ("ep", "ta", "tb"), EP * TA * TB)
    mixed = combine(returned, coef_hi, coef_lo, own)
    return (mixed, new_keys, new_values)


def solution(mesh):
    cut = Mesh(mesh.devices.reshape(EP, TA, TB), ("ep", "ta", "tb"))
    tp = ("ta", "tb")
    placed = (
        P("ep", None),
        P(),
        P(None, tp),
        P(None, tp),
        P(None, tp),
        P(),
        P(),
        P(tp),
        P("ep", None, tp),
        P("ep", None, tp),
        P("ep"),
        P(tp, None),
        P(),
        P("ep", None),
        P("ep", None),
        P(("ep", "ta", "tb"), None, None),
        P(("ep", "ta", "tb"), None, None),
        P(("ep", "ta", "tb"), None, None),
        P(None, tp),
        P(None, tp),
        P(tp, None),
    )
    return jax.shard_map(
        local,
        mesh=cut,
        in_specs=placed,
        out_specs=(P("ep", tp),) * 3,
        check_vma=False,
    )
```

```python
import jax
import jax.numpy as jnp
from jax import lax
from jax.experimental import pallas as pl
from jax.experimental.pallas import tpu as pltpu
from jax.sharding import Mesh, PartitionSpec as P

EPS = 1e-06
BF16 = jnp.bfloat16
F32 = jnp.float32
LANES = 128
EP, TA, TB = 16, 4, 4
ROWS = 16
SLOTS = 4
LATE = 7
BLOCKS = 16
MIB = 1024 * 1024


def rms_rows(values, gain):
    mean_sq = jnp.mean(values * values, axis=-1, keepdims=True)
    return values * lax.rsqrt(mean_sq + EPS) * gain


def dot(x, w):
    return jnp.dot(x, w, preferred_element_type=F32)


def dot_nt(x, w):
    return lax.dot_general(x, w, (((1,), (1,)), ((), ())), preferred_element_type=F32)


def vmem():
    return pl.BlockSpec(memory_space=pltpu.VMEM)


def hbm():
    return pl.BlockSpec(memory_space=pltpu.HBM)


def route_tables(routes, weights, a, pick_ref, coef_hi_ref, coef_lo_ref):
    experts = EP * TA
    expert_ids = lax.broadcasted_iota(jnp.int32, (experts, ROWS), 0)
    member = jnp.zeros((experts, ROWS), F32)
    weight_of = jnp.zeros((experts, ROWS), F32)
    for k in range(routes.shape[0]):
        hit = routes[k : k + 1, :] == expert_ids
        member = member + jnp.where(hit, 1.0, 0.0)
        weight_of = weight_of + jnp.where(hit, weights[k : k + 1, :], 0.0)
    row_in = lax.broadcasted_iota(jnp.int32, (ROWS, ROWS), 0)
    row_out = lax.broadcasted_iota(jnp.int32, (ROWS, ROWS), 1)
    rank = dot(member.astype(BF16), (row_in < row_out).astype(F32).astype(BF16))
    slot_of = (member * (rank + 1.0)).astype(BF16)

    count = EP * TB * TA * SLOTS
    wide_in = lax.broadcasted_iota(jnp.int32, (ROWS, 64), 0)
    wide_out = lax.broadcasted_iota(jnp.int32, (ROWS, 64), 1)
    widen = (wide_out % ROWS == wide_in).astype(F32).astype(BF16)
    row = lax.broadcasted_iota(jnp.int32, (count, 64), 0)
    lane = lax.broadcasted_iota(jnp.int32, (count, 64), 1)
    owner = (lane == (row // 64) * TA + a).astype(F32).astype(BF16)
    found = dot(owner, dot(slot_of, widen).astype(BF16))
    slot = row % SLOTS
    same_block = (row // SLOTS) % TA == lane // ROWS
    routed = found == (slot + 1).astype(F32)
    shared = lane % ROWS == row // 64
    chosen = jnp.where(slot == SLOTS - 1, shared.astype(F32), routed.astype(F32))
    pick_ref[...] = jnp.where(same_block, chosen, 0.0).astype(BF16)

    turn = (row_in == row_out).astype(F32).astype(BF16)
    spread_row = lax.broadcasted_iota(jnp.int32, (experts, count), 0)
    spread_lane = lax.broadcasted_iota(jnp.int32, (experts, count), 1)
    spread = (spread_row == spread_lane // 16).astype(F32).astype(BF16)
    hi = weight_of.astype(BF16)
    lo = (weight_of - hi.astype(F32)).astype(BF16)
    turned = dot_nt(turn, jnp.concatenate([slot_of, hi, lo], axis=0)).astype(BF16)
    by_col = dot(
        jnp.concatenate([turned[:, n * experts : (n + 1) * experts] for n in range(3)], axis=0),
        spread,
    )
    col = lax.broadcasted_iota(jnp.int32, (ROWS, count), 1)
    token = lax.broadcasted_iota(jnp.int32, (ROWS, count), 0)
    col_slot = col % SLOTS
    held = by_col[:ROWS] == (col_slot + 1).astype(F32)
    is_shared = col_slot == SLOTS - 1
    own_shared = (token == col // 64).astype(F32)
    coef_hi_ref[...] = jnp.where(
        is_shared, own_shared, jnp.where(held, by_col[ROWS : 2 * ROWS], 0.0)
    ).astype(BF16)
    coef_lo_ref[...] = jnp.where(is_shared | ~held, 0.0, by_col[2 * ROWS :]).astype(BF16)


def attention_kernel(
    bias_hbm,
    lengths_hbm,
    norm_gain_hbm,
    query_gain_hbm,
    key_gain_hbm,
    routes_hbm,
    route_weight_hbm,
    tokens_hbm,
    wq_hbm,
    wk_hbm,
    wv_hbm,
    key_hbm,
    value_hbm,
    wout_hbm,
    *rest,
):
    late_hbm, rest = rest[:LATE], rest[LATE:]
    (
    out_ref,
    new_keys_hbm,
    new_values_hbm,
    tok_slice_ref,
    pick_ref,
    coef_hi_ref,
    coef_lo_ref,
    *rest,
    ) = rest
    late_refs, rest = rest[:LATE], rest[LATE:]
    (
    bias_buf,
    lengths_buf,
    norm_gain_buf,
    query_gain_buf,
    key_gain_buf,
    routes_buf,
    route_weight_buf,
    tokens_buf,
    wq_buf,
    wk_buf,
    wv_buf,
    key_buf,
    value_buf,
    wout_buf,
    q_buf,
    z_buf,
    w_buf,
    att_buf,
    length_rows,
    new_keys_buf,
    new_values_buf,
    small_sem,
    sem,
    key_sem,
    value_sem,
    out_sem,
    late_sem,
    ) = rest
    a, b = lax.axis_index("ta"), lax.axis_index("tb")
    small = [
        pltpu.make_async_copy(src, dst, small_sem.at[n])
        for n, (src, dst) in enumerate(
            (
                (lengths_hbm, lengths_buf),
                (bias_hbm, bias_buf),
                (routes_hbm, routes_buf),
                (route_weight_hbm, route_weight_buf),
                (norm_gain_hbm, norm_gain_buf),
                (query_gain_hbm, query_gain_buf),
                (key_gain_hbm, key_gain_buf),
            )
        )
    ]
    large = [
        pltpu.make_async_copy(src, dst, sem.at[n])
        for n, (src, dst) in enumerate(
            (
                (tokens_hbm, tokens_buf),
                (wq_hbm, wq_buf),
                (wk_hbm, wk_buf),
                (wv_hbm, wv_buf),
                (wout_hbm, wout_buf),
            )
        )
    ]
    late = [
        pltpu.make_async_copy(src, dst, late_sem.at[n])
        for n, (src, dst) in enumerate(zip(late_hbm, late_refs))
    ]
    cache_len = key_buf.shape[1]
    head_size = key_buf.shape[2]
    key_head = pltpu.make_async_copy(key_hbm, key_buf, key_sem.at[ROWS])
    value_copies = [pltpu.make_async_copy(value_hbm, value_buf, value_sem.at[ROWS])]
    for copy in small + large[:4] + [key_head] + value_copies + large[4:] + late:
        copy.start()

    for copy in small + large[:4]:
        copy.wait()
    for s in range(ROWS):
        length_rows[s : s + 1, :] = jnp.full((1, LANES), lengths_buf[s], jnp.int32)
    normed = rms_rows(tokens_buf[...].astype(F32), norm_gain_buf[...]).astype(BF16)
    q_buf[...] = (
        rms_rows(dot(normed, wq_buf[...]), query_gain_buf[...]).astype(BF16).astype(F32)
    )
    new_keys_buf[...] = rms_rows(dot(normed, wk_buf[...]), key_gain_buf[...]).astype(BF16)
    new_values_buf[...] = dot(normed, wv_buf[...]).astype(BF16)
    out_copies = [
        pltpu.make_async_copy(new_keys_buf, new_keys_hbm, out_sem.at[0]),
        pltpu.make_async_copy(new_values_buf, new_values_hbm, out_sem.at[1]),
    ]
    for copy in out_copies:
        copy.start()
    route_tables(
        routes_buf[...], route_weight_buf[...], a, pick_ref, coef_hi_ref, coef_lo_ref
    )
    for j in range(TA):
        cols = pl.ds(pl.multiple_of((j * TB + b) * LANES, LANES), LANES)
        tok_slice_ref[j * ROWS : (j + 1) * ROWS, :] = tokens_buf[:, cols].astype(F32)

    key_head.wait()
    for s in range(ROWS):
        z_buf[s : s + 1, :] = dot_nt(q_buf[s : s + 1, :].astype(BF16), key_buf[s])

    chunks = cache_len // LANES
    after = lax.broadcasted_iota(jnp.int32, (3 * LANES, LANES), 0) % LANES
    upto = lax.broadcasted_iota(jnp.int32, (3 * LANES, LANES), 1)
    later = (after > upto).astype(F32).astype(BF16)
    chunk_lane = lax.broadcasted_iota(jnp.int32, (ROWS, LANES), 1)
    logits = z_buf[...] * head_size ** (-0.5) + bias_buf[0, 0]
    soft = jnp.log1p(jnp.exp(-jnp.abs(logits)))
    log_beta = jnp.minimum(logits, 0.0) - soft
    log_not = jnp.minimum(-logits, 0.0) - soft
    visible = [chunk_lane + c * LANES < length_rows[...] for c in range(chunks)]
    stacked = jnp.concatenate(
        [
            jnp.where(visible[c], log_not[:, c * LANES : (c + 1) * LANES], 0.0)
            for c in range(chunks)
        ],
        axis=0,
    )
    first = stacked.astype(BF16)
    rest = stacked - first.astype(F32)
    second = rest.astype(BF16)
    third = (rest - second.astype(F32)).astype(BF16)
    inner = dot(jnp.concatenate([first, second, third], axis=1), later)
    totals = jnp.sum(stacked, axis=1, keepdims=True)
    carry = jnp.zeros((ROWS, 1), F32)
    for c in reversed(range(chunks)):
        cols = slice(c * LANES, (c + 1) * LANES)
        later_sum = inner[c * ROWS : (c + 1) * ROWS, :] + carry
        w_buf[:, cols] = jnp.where(visible[c], jnp.exp(log_beta[:, cols] + later_sum), 0.0)
        carry = carry + totals[c * ROWS : (c + 1) * ROWS, :]

    for copy in value_copies + large[4:]:
        copy.wait()
    for s in range(ROWS):
        att_buf[s : s + 1, :] = dot(w_buf[s : s + 1, :].astype(BF16), value_buf[s])
    attn = dot(att_buf[...].astype(BF16), wout_buf[...]).astype(BF16)
    for t in range(BLOCKS):
        block = attn[:, t * LANES : (t + 1) * LANES]
        j, quarter = t // TB, t % TB
        for n in range(TA):
            start = (n * TB + quarter) * 64 + j * ROWS
            out_ref[start : start + ROWS, :] = block
    for copy in out_copies + late:
        copy.wait()


def attention(
    bias,
    lengths,
    norm_gain,
    query_gain,
    key_gain,
    routes,
    route_weight,
    tokens,
    wq,
    wk,
    wv,
    keys,
    values,
    wout,
    *late,
):
    rows, cache_len, head_size = keys.shape
    width = tokens.shape[1]
    shape = jax.ShapeDtypeStruct
    return pl.pallas_call(
        attention_kernel,
        name="attention",
        out_shape=(
            shape((1024, LANES), BF16),
            shape((rows, head_size), BF16),
            shape((rows, head_size), BF16),
            shape((64, LANES), F32),
            shape((1024, 64), BF16),
            shape((rows, 1024), BF16),
            shape((rows, 1024), BF16),
            *(shape(x.shape, x.dtype) for x in late),
        ),
        in_specs=[hbm()] * (14 + LATE),
        out_specs=(vmem(), hbm(), hbm()) + (vmem(),) * (4 + LATE),
        scratch_shapes=[
            pltpu.SMEM(bias.shape, F32),
            pltpu.SMEM(lengths.shape, jnp.int32),
            pltpu.VMEM(norm_gain.shape, F32),
            pltpu.VMEM(query_gain.shape, F32),
            pltpu.VMEM(key_gain.shape, F32),
            pltpu.VMEM(routes.shape, jnp.int32),
            pltpu.VMEM(route_weight.shape, F32),
            pltpu.VMEM((rows, width), BF16),
            pltpu.VMEM((width, head_size), BF16),
            pltpu.VMEM((width, head_size), BF16),
            pltpu.VMEM((width, head_size), BF16),
            pltpu.VMEM((rows, cache_len, head_size), BF16),
            pltpu.VMEM((rows, cache_len, head_size), BF16),
            pltpu.VMEM((head_size, width), BF16),
            pltpu.VMEM((rows, head_size), F32),
            pltpu.VMEM((rows, cache_len), F32),
            pltpu.VMEM((rows, cache_len), F32),
            pltpu.VMEM((rows, head_size), F32),
            pltpu.VMEM((rows, LANES), jnp.int32),
            pltpu.VMEM((rows, head_size), BF16),
            pltpu.VMEM((rows, head_size), BF16),
            pltpu.SemaphoreType.DMA((7,)),
            pltpu.SemaphoreType.DMA((5,)),
            pltpu.SemaphoreType.DMA((rows + 1,)),
            pltpu.SemaphoreType.DMA((rows + 1,)),
            pltpu.SemaphoreType.DMA((2,)),
            pltpu.SemaphoreType.DMA((LATE,)),
        ],
        cost_estimate=pl.CostEstimate(
            flops=2_000_000_000, bytes_accessed=10 * MIB, transcendentals=0
        ),
        compiler_params=pltpu.CompilerParams(vmem_limit_bytes=16 * MIB),
    )(
        bias,
        *(pltpu.with_memory_space_constraint(x, pltpu.HBM) for x in (
        lengths,
        norm_gain,
        query_gain,
        key_gain,
        routes,
        route_weight,
        tokens,
        wq,
        wk,
        wv,
        keys,
        values,
        wout,
        *late,
        ))
    )


def dispatch_kernel(arrived_ref, tok_slice_ref, pick_ref, out_ref, own_ref, h_buf):
    total = tok_slice_ref[...]
    parts = [arrived_ref[n * 64 : (n + 1) * 64, :].astype(F32) for n in range(TA * TB)]
    while len(parts) > 1:
        parts = [parts[n] + parts[n + 1] for n in range(0, len(parts), 2)]
    h = (total + parts[0]).astype(BF16)
    h_buf[...] = h.astype(F32)
    out_ref[...] = dot(pick_ref[...], h).astype(BF16)
    own_ref[...] = h_buf[pl.ds(pl.multiple_of(lax.axis_index("ta") * ROWS, ROWS), ROWS), :]


def dispatch(arrived, tok_slice, pick):
    shape = jax.ShapeDtypeStruct
    return pl.pallas_call(
        dispatch_kernel,
        name="dispatch",
        out_shape=(shape((1024, LANES), BF16), shape((ROWS, LANES), F32)),
        in_specs=[vmem()] * 3,
        out_specs=(vmem(),) * 2,
        scratch_shapes=[pltpu.VMEM((64, LANES), F32)],
        cost_estimate=pl.CostEstimate(
            flops=500_000_000, bytes_accessed=MIB, transcendentals=0
        ),
        compiler_params=pltpu.CompilerParams(vmem_limit_bytes=4 * MIB),
    )(arrived, tok_slice, pick)


def expert_kernel(
    arrived_ref,
    post_gain_ref,
    gate_ref,
    up_ref,
    down_ref,
    shared_gate_ref,
    shared_up_ref,
    shared_down_ref,
    out_ref,
    rows_buf,
    x_buf,
    send_buf,
):
    rows_buf[...] = arrived_ref[...].astype(F32)
    for t in range(BLOCKS):
        j, b = t // TB, t % TB
        for s in range(SLOTS):
            x_buf[s * ROWS : (s + 1) * ROWS, t * LANES : (t + 1) * LANES] = rows_buf[
                pl.ds(b * 16 + j * SLOTS + s, EP, stride=64), :
            ]
    h_normed = rms_rows(x_buf[...], post_gain_ref[...]).astype(BF16)
    routed_rows, shared_rows = h_normed[:48], h_normed[48:]
    gate = dot(routed_rows, gate_ref[...])
    up = dot(routed_rows, up_ref[...])
    hidden = (gate * jax.nn.sigmoid(gate) * up).astype(BF16)
    s_gate = dot_nt(shared_rows, shared_gate_ref[...])
    s_up = dot_nt(shared_rows, shared_up_ref[...])
    s_hidden = (s_gate * jax.nn.sigmoid(s_gate) * s_up).astype(BF16)
    routed = dot(hidden, down_ref[...])
    shared = dot(s_hidden, shared_down_ref[...])
    for t in range(BLOCKS):
        cols = slice(t * LANES, (t + 1) * LANES)
        for s in range(SLOTS):
            part = routed[s * ROWS : (s + 1) * ROWS, cols] if s < SLOTS - 1 else shared[:, cols]
            send_buf[pl.ds(t * SLOTS + s, EP, stride=64), :] = part
    out_ref[...] = send_buf[...].astype(BF16)


def run_experts(arrived, post_gain, gate, up, down, s_gate, s_up, s_down):
    return pl.pallas_call(
        expert_kernel,
        name="experts",
        out_shape=jax.ShapeDtypeStruct((1024, LANES), BF16),
        in_specs=[vmem()] * 8,
        out_specs=vmem(),
        scratch_shapes=[
            pltpu.VMEM((1024, LANES), F32),
            pltpu.VMEM((64, BLOCKS * LANES), F32),
            pltpu.VMEM((1024, LANES), F32),
        ],
        cost_estimate=pl.CostEstimate(
            flops=1_000_000_000, bytes_accessed=3 * MIB, transcendentals=0
        ),
        compiler_params=pltpu.CompilerParams(vmem_limit_bytes=12 * MIB),
    )(arrived, post_gain, gate, up, down, s_gate, s_up, s_down)


def combine_kernel(arrived_ref, coef_hi_ref, coef_lo_ref, own_ref, out_ref):
    arrived = arrived_ref[...]
    both = dot(jnp.concatenate([coef_hi_ref[...], coef_lo_ref[...]], axis=0), arrived)
    out_ref[...] = (own_ref[...] + (both[:ROWS] + both[ROWS:])).astype(BF16)


def combine(arrived, coef_hi, coef_lo, own):
    return pl.pallas_call(
        combine_kernel,
        name="combine",
        out_shape=jax.ShapeDtypeStruct((ROWS, LANES), BF16),
        in_specs=[vmem()] * 4,
        out_specs=vmem(),
        cost_estimate=pl.CostEstimate(
            flops=100_000_000, bytes_accessed=MIB, transcendentals=0
        ),
        compiler_params=pltpu.CompilerParams(vmem_limit_bytes=4 * MIB),
    )(arrived, coef_hi, coef_lo, own)


def exchange(x, axes, parts):
    pieces = x.reshape(parts, -1, LANES)
    arrived = lax.all_to_all(pieces, axes, split_axis=0, concat_axis=0, tiled=True)
    return arrived.reshape(x.shape)


def local(
    tokens,
    norm_gain,
    w_query,
    w_key,
    w_value,
    query_gain,
    key_gain,
    score_bias,
    key_cache,
    value_cache,
    lengths,
    w_out,
    post_gain,
    routes,
    route_weight,
    expert_gate,
    expert_up,
    expert_down,
    shared_gate,
    shared_up,
    shared_down,
):
    partial_rows, new_keys, new_values, tok_slice, pick, coef_hi, coef_lo, *late = attention(
        score_bias[None, :],
        lengths,
        norm_gain[None, :],
        query_gain[None, :],
        key_gain[None, :],
        routes.T,
        route_weight.T,
        tokens,
        w_query,
        w_key,
        w_value,
        key_cache,
        value_cache,
        w_out,
        post_gain[None, :],
        expert_gate[0],
        expert_up[0],
        expert_down[0],
        shared_gate.T,
        shared_up.T,
        shared_down,
    )
    arrived = exchange(partial_rows, ("ta", "tb"), TA * TB)
    outgoing, own = dispatch(arrived, tok_slice, pick)
    received = exchange(outgoing, ("ep", "tb"), EP * TB)
    parts = run_experts(received, *late)
    returned = exchange(parts, ("ep", "ta", "tb"), EP * TA * TB)
    mixed = combine(returned, coef_hi, coef_lo, own)
    return (mixed, new_keys, new_values)


def solution(mesh):
    cut = Mesh(mesh.devices.reshape(EP, TA, TB), ("ep", "ta", "tb"))
    tp = ("ta", "tb")
    placed = (
        P("ep", None),
        P(),
        P(None, tp),
        P(None, tp),
        P(None, tp),
        P(),
        P(),
        P(tp),
        P("ep", None, tp),
        P("ep", None, tp),
        P("ep"),
        P(tp, None),
        P(),
        P("ep", None),
        P("ep", None),
        P(("ep", "ta", "tb"), None, None),
        P(("ep", "ta", "tb"), None, None),
        P(("ep", "ta", "tb"), None, None),
        P(None, tp),
        P(None, tp),
        P(tp, None),
    )
    return jax.shard_map(
        local,
        mesh=cut,
        in_specs=placed,
        out_specs=(P("ep", tp),) * 3,
        check_vma=False,
    )
```

```python
import jax
import jax.numpy as jnp
from jax import lax
from jax.experimental import pallas as pl
from jax.experimental.pallas import tpu as pltpu
from jax.sharding import Mesh, PartitionSpec as P

EPS = 1e-06
BF16 = jnp.bfloat16
F32 = jnp.float32
LANES = 128
EP, TA, TB = 16, 4, 4
ROWS = 16
SLOTS = 4
SMALL = 6
LATE = 10
BLOCKS = 16
MIB = 1024 * 1024


def rms_rows(values, gain):
    mean_sq = jnp.mean(values * values, axis=-1, keepdims=True)
    return values * lax.rsqrt(mean_sq + EPS) * gain


def dot(x, w):
    return jnp.dot(x, w, preferred_element_type=F32)


def dot_nt(x, w):
    return lax.dot_general(x, w, (((1,), (1,)), ((), ())), preferred_element_type=F32)


def vmem():
    return pl.BlockSpec(memory_space=pltpu.VMEM)


def hbm():
    return pl.BlockSpec(memory_space=pltpu.HBM)


def route_tables(routes, weights, a, pick_ref, coef_hi_ref, coef_lo_ref):
    experts = EP * TA
    expert_ids = lax.broadcasted_iota(jnp.int32, (experts, ROWS), 0)
    member = jnp.zeros((experts, ROWS), F32)
    weight_of = jnp.zeros((experts, ROWS), F32)
    for k in range(routes.shape[0]):
        hit = routes[k : k + 1, :] == expert_ids
        member = member + jnp.where(hit, 1.0, 0.0)
        weight_of = weight_of + jnp.where(hit, weights[k : k + 1, :], 0.0)
    row_in = lax.broadcasted_iota(jnp.int32, (ROWS, ROWS), 0)
    row_out = lax.broadcasted_iota(jnp.int32, (ROWS, ROWS), 1)
    rank = dot(member.astype(BF16), (row_in < row_out).astype(F32).astype(BF16))
    slot_of = (member * (rank + 1.0)).astype(BF16)

    count = EP * TB * TA * SLOTS
    wide_in = lax.broadcasted_iota(jnp.int32, (ROWS, 64), 0)
    wide_out = lax.broadcasted_iota(jnp.int32, (ROWS, 64), 1)
    widen = (wide_out % ROWS == wide_in).astype(F32).astype(BF16)
    row = lax.broadcasted_iota(jnp.int32, (count, 64), 0)
    lane = lax.broadcasted_iota(jnp.int32, (count, 64), 1)
    owner = (lane == (row // 64) * TA + a).astype(F32).astype(BF16)
    found = dot(owner, dot(slot_of, widen).astype(BF16))
    slot = row % SLOTS
    same_block = (row // SLOTS) % TA == lane // ROWS
    routed = found == (slot + 1).astype(F32)
    shared = lane % ROWS == row // 64
    chosen = jnp.where(slot == SLOTS - 1, shared.astype(F32), routed.astype(F32))
    pick_ref[...] = jnp.where(same_block, chosen, 0.0).astype(BF16)

    turn = (row_in == row_out).astype(F32).astype(BF16)
    spread_row = lax.broadcasted_iota(jnp.int32, (experts, count), 0)
    spread_lane = lax.broadcasted_iota(jnp.int32, (experts, count), 1)
    spread = (spread_row == spread_lane // 16).astype(F32).astype(BF16)
    hi = weight_of.astype(BF16)
    lo = (weight_of - hi.astype(F32)).astype(BF16)
    turned = dot_nt(turn, jnp.concatenate([slot_of, hi, lo], axis=0)).astype(BF16)
    by_col = dot(
        jnp.concatenate([turned[:, n * experts : (n + 1) * experts] for n in range(3)], axis=0),
        spread,
    )
    col = lax.broadcasted_iota(jnp.int32, (ROWS, count), 1)
    token = lax.broadcasted_iota(jnp.int32, (ROWS, count), 0)
    col_slot = col % SLOTS
    held = by_col[:ROWS] == (col_slot + 1).astype(F32)
    is_shared = col_slot == SLOTS - 1
    own_shared = (token == col // 64).astype(F32)
    coef_hi_ref[...] = jnp.where(
        is_shared, own_shared, jnp.where(held, by_col[ROWS : 2 * ROWS], 0.0)
    ).astype(BF16)
    coef_lo_ref[...] = jnp.where(is_shared | ~held, 0.0, by_col[2 * ROWS :]).astype(BF16)


def attention_kernel(*refs):
    small_hbm, refs = refs[:SMALL], refs[SMALL:]
    tokens_hbm, wq_hbm, key_hbm, value_hbm, wout_hbm, *refs = refs
    late_hbm, refs = refs[:LATE], refs[LATE:]
    out_ref, normed_ref, tok_slice_ref, pick_ref, coef_hi_ref, coef_lo_ref, *refs = refs
    late_refs, refs = refs[:LATE], refs[LATE:]
    small_bufs, refs = refs[:SMALL], refs[SMALL:]
    tokens_buf, wq_buf, key_buf, value_buf, wout_buf, *refs = refs
    q_buf, z_buf, w_buf, att_buf, length_rows, small_sem, sem, late_sem = refs
    lengths_buf, bias_buf, routes_buf, route_weight_buf, norm_gain_buf, query_gain_buf = small_bufs
    a, b = lax.axis_index("ta"), lax.axis_index("tb")
    small = [
        pltpu.make_async_copy(src, dst, small_sem.at[n])
        for n, (src, dst) in enumerate(zip(small_hbm, small_bufs))
    ]
    tokens_copy, wq_copy, key_copy, value_copy, wout_copy = large = [
        pltpu.make_async_copy(src, dst, sem.at[n])
        for n, (src, dst) in enumerate(
            (
                (tokens_hbm, tokens_buf),
                (wq_hbm, wq_buf),
                (key_hbm, key_buf),
                (value_hbm, value_buf),
                (wout_hbm, wout_buf),
            )
        )
    ]
    late = [
        pltpu.make_async_copy(src, dst, late_sem.at[n])
        for n, (src, dst) in enumerate(zip(late_hbm, late_refs))
    ]
    for copy in small + large + late:
        copy.start()

    cache_len = key_buf.shape[1]
    head_size = key_buf.shape[2]
    for copy in small + [tokens_copy, wq_copy]:
        copy.wait()
    for s in range(ROWS):
        length_rows[s : s + 1, :] = jnp.full((1, LANES), lengths_buf[s], jnp.int32)
    normed = rms_rows(tokens_buf[...].astype(F32), norm_gain_buf[...]).astype(BF16)
    q_buf[...] = (
        rms_rows(dot(normed, wq_buf[...]), query_gain_buf[...]).astype(BF16).astype(F32)
    )
    normed_ref[...] = normed
    route_tables(
        routes_buf[...], route_weight_buf[...], a, pick_ref, coef_hi_ref, coef_lo_ref
    )
    for j in range(TA):
        cols = pl.ds(pl.multiple_of((j * TB + b) * LANES, LANES), LANES)
        tok_slice_ref[j * ROWS : (j + 1) * ROWS, :] = tokens_buf[:, cols].astype(F32)

    key_copy.wait()
    for s in range(ROWS):
        z_buf[s : s + 1, :] = dot_nt(q_buf[s : s + 1, :].astype(BF16), key_buf[s])

    chunks = cache_len // LANES
    after = lax.broadcasted_iota(jnp.int32, (3 * LANES, LANES), 0) % LANES
    upto = lax.broadcasted_iota(jnp.int32, (3 * LANES, LANES), 1)
    later = (after > upto).astype(F32).astype(BF16)
    chunk_lane = lax.broadcasted_iota(jnp.int32, (ROWS, LANES), 1)
    logits = z_buf[...] * head_size ** (-0.5) + bias_buf[0, 0]
    soft = jnp.log1p(jnp.exp(-jnp.abs(logits)))
    log_beta = jnp.minimum(logits, 0.0) - soft
    log_not = jnp.minimum(-logits, 0.0) - soft
    visible = [chunk_lane + c * LANES < length_rows[...] for c in range(chunks)]
    stacked = jnp.concatenate(
        [
            jnp.where(visible[c], log_not[:, c * LANES : (c + 1) * LANES], 0.0)
            for c in range(chunks)
        ],
        axis=0,
    )
    first = stacked.astype(BF16)
    rest = stacked - first.astype(F32)
    second = rest.astype(BF16)
    third = (rest - second.astype(F32)).astype(BF16)
    inner = dot(jnp.concatenate([first, second, third], axis=1), later)
    totals = jnp.sum(stacked, axis=1, keepdims=True)
    carry = jnp.zeros((ROWS, 1), F32)
    for c in reversed(range(chunks)):
        cols = slice(c * LANES, (c + 1) * LANES)
        later_sum = inner[c * ROWS : (c + 1) * ROWS, :] + carry
        w_buf[:, cols] = jnp.where(visible[c], jnp.exp(log_beta[:, cols] + later_sum), 0.0)
        carry = carry + totals[c * ROWS : (c + 1) * ROWS, :]

    value_copy.wait()
    wout_copy.wait()
    for s in range(ROWS):
        att_buf[s : s + 1, :] = dot(w_buf[s : s + 1, :].astype(BF16), value_buf[s])
    attn = dot(att_buf[...].astype(BF16), wout_buf[...]).astype(BF16)
    for t in range(BLOCKS):
        block = attn[:, t * LANES : (t + 1) * LANES]
        j, quarter = t // TB, t % TB
        for n in range(TA):
            start = (n * TB + quarter) * 64 + j * ROWS
            out_ref[start : start + ROWS, :] = block
    for copy in late:
        copy.wait()


def attention(small, tokens, wq, keys, values, wout, late):
    rows, cache_len, head_size = keys.shape
    width = tokens.shape[1]
    shape = jax.ShapeDtypeStruct
    kept = [pltpu.with_memory_space_constraint(x, pltpu.HBM) for x in small if x.size > 1]
    small = (kept[0], small[1], *kept[1:])
    large = (tokens, wq, keys, values, wout, *late)
    return pl.pallas_call(
        attention_kernel,
        name="attention",
        out_shape=(
            shape((1024, LANES), BF16),
            shape((rows, width), BF16),
            shape((64, LANES), F32),
            shape((1024, 64), BF16),
            shape((rows, 1024), BF16),
            shape((rows, 1024), BF16),
            *(shape(x.shape, x.dtype) for x in late),
        ),
        in_specs=[hbm()] * (SMALL + 5 + LATE),
        out_specs=(vmem(),) * (6 + LATE),
        scratch_shapes=[
            pltpu.SMEM(small[0].shape, jnp.int32),
            pltpu.SMEM(small[1].shape, F32),
            *(pltpu.VMEM(x.shape, x.dtype) for x in small[2:]),
            pltpu.VMEM((rows, width), BF16),
            pltpu.VMEM((width, head_size), BF16),
            pltpu.VMEM((rows, cache_len, head_size), BF16),
            pltpu.VMEM((rows, cache_len, head_size), BF16),
            pltpu.VMEM((head_size, width), BF16),
            pltpu.VMEM((rows, head_size), F32),
            pltpu.VMEM((rows, cache_len), F32),
            pltpu.VMEM((rows, cache_len), F32),
            pltpu.VMEM((rows, head_size), F32),
            pltpu.VMEM((rows, LANES), jnp.int32),
            pltpu.SemaphoreType.DMA((SMALL,)),
            pltpu.SemaphoreType.DMA((5,)),
            pltpu.SemaphoreType.DMA((LATE,)),
        ],
        cost_estimate=pl.CostEstimate(
            flops=2_000_000_000, bytes_accessed=12 * MIB, transcendentals=0
        ),
        compiler_params=pltpu.CompilerParams(vmem_limit_bytes=16 * MIB),
    )(*small, *(pltpu.with_memory_space_constraint(x, pltpu.HBM) for x in large))


def dispatch_kernel(arrived_ref, tok_slice_ref, pick_ref, out_ref, own_ref, h_buf):
    total = tok_slice_ref[...]
    parts = [arrived_ref[n * 64 : (n + 1) * 64, :].astype(F32) for n in range(TA * TB)]
    while len(parts) > 1:
        parts = [parts[n] + parts[n + 1] for n in range(0, len(parts), 2)]
    h = (total + parts[0]).astype(BF16)
    h_buf[...] = h.astype(F32)
    out_ref[...] = dot(pick_ref[...], h).astype(BF16)
    own_ref[...] = h_buf[pl.ds(pl.multiple_of(lax.axis_index("ta") * ROWS, ROWS), ROWS), :]


def dispatch(arrived, tok_slice, pick):
    shape = jax.ShapeDtypeStruct
    return pl.pallas_call(
        dispatch_kernel,
        name="dispatch",
        out_shape=(shape((1024, LANES), BF16), shape((ROWS, LANES), F32)),
        in_specs=[vmem()] * 3,
        out_specs=(vmem(),) * 2,
        scratch_shapes=[pltpu.VMEM((64, LANES), F32)],
        cost_estimate=pl.CostEstimate(
            flops=500_000_000, bytes_accessed=MIB, transcendentals=0
        ),
        compiler_params=pltpu.CompilerParams(vmem_limit_bytes=4 * MIB),
    )(arrived, tok_slice, pick)


def expert_kernel(
    arrived_ref,
    normed_ref,
    post_gain_ref,
    gate_ref,
    up_ref,
    down_ref,
    shared_gate_ref,
    shared_up_ref,
    shared_down_ref,
    wk_ref,
    wv_ref,
    key_gain_ref,
    out_ref,
    new_keys_hbm,
    new_values_hbm,
    rows_buf,
    x_buf,
    send_buf,
    new_keys_buf,
    new_values_buf,
    sem,
):
    normed = normed_ref[...]
    new_keys_buf[...] = rms_rows(dot(normed, wk_ref[...]), key_gain_ref[...]).astype(BF16)
    new_values_buf[...] = dot(normed, wv_ref[...]).astype(BF16)
    copies = [
        pltpu.make_async_copy(new_keys_buf, new_keys_hbm, sem.at[0]),
        pltpu.make_async_copy(new_values_buf, new_values_hbm, sem.at[1]),
    ]
    for copy in copies:
        copy.start()
    rows_buf[...] = arrived_ref[...].astype(F32)
    for t in range(BLOCKS):
        j, b = t // TB, t % TB
        for s in range(SLOTS):
            x_buf[s * ROWS : (s + 1) * ROWS, t * LANES : (t + 1) * LANES] = rows_buf[
                pl.ds(b * 16 + j * SLOTS + s, EP, stride=64), :
            ]
    h_normed = rms_rows(x_buf[...], post_gain_ref[...]).astype(BF16)
    routed_rows, shared_rows = h_normed[:48], h_normed[48:]
    gate = dot(routed_rows, gate_ref[...])
    up = dot(routed_rows, up_ref[...])
    hidden = (gate * jax.nn.sigmoid(gate) * up).astype(BF16)
    s_gate = dot_nt(shared_rows, shared_gate_ref[...])
    s_up = dot_nt(shared_rows, shared_up_ref[...])
    s_hidden = (s_gate * jax.nn.sigmoid(s_gate) * s_up).astype(BF16)
    routed = dot(hidden, down_ref[...])
    shared = dot(s_hidden, shared_down_ref[...])
    for t in range(BLOCKS):
        cols = slice(t * LANES, (t + 1) * LANES)
        for s in range(SLOTS):
            part = routed[s * ROWS : (s + 1) * ROWS, cols] if s < SLOTS - 1 else shared[:, cols]
            send_buf[pl.ds(t * SLOTS + s, EP, stride=64), :] = part
    out_ref[...] = send_buf[...].astype(BF16)
    for copy in copies:
        copy.wait()


def run_experts(arrived, normed, *late):
    shape = jax.ShapeDtypeStruct
    rows = normed.shape[0]
    return pl.pallas_call(
        expert_kernel,
        name="experts",
        out_shape=(
            shape((1024, LANES), BF16),
            shape((rows, LANES), BF16),
            shape((rows, LANES), BF16),
        ),
        in_specs=[vmem()] * (2 + LATE),
        out_specs=(vmem(), hbm(), hbm()),
        scratch_shapes=[
            pltpu.VMEM((1024, LANES), F32),
            pltpu.VMEM((64, BLOCKS * LANES), F32),
            pltpu.VMEM((1024, LANES), F32),
            pltpu.VMEM((rows, LANES), BF16),
            pltpu.VMEM((rows, LANES), BF16),
            pltpu.SemaphoreType.DMA((2,)),
        ],
        cost_estimate=pl.CostEstimate(
            flops=1_000_000_000, bytes_accessed=3 * MIB, transcendentals=0
        ),
        compiler_params=pltpu.CompilerParams(vmem_limit_bytes=12 * MIB),
    )(arrived, normed, *late)


def combine_kernel(arrived_ref, coef_hi_ref, coef_lo_ref, own_ref, out_ref):
    arrived = arrived_ref[...]
    both = dot(jnp.concatenate([coef_hi_ref[...], coef_lo_ref[...]], axis=0), arrived)
    out_ref[...] = (own_ref[...] + (both[:ROWS] + both[ROWS:])).astype(BF16)


def combine(arrived, coef_hi, coef_lo, own):
    return pl.pallas_call(
        combine_kernel,
        name="combine",
        out_shape=jax.ShapeDtypeStruct((ROWS, LANES), BF16),
        in_specs=[vmem()] * 4,
        out_specs=vmem(),
        cost_estimate=pl.CostEstimate(
            flops=100_000_000, bytes_accessed=MIB, transcendentals=0
        ),
        compiler_params=pltpu.CompilerParams(vmem_limit_bytes=4 * MIB),
    )(arrived, coef_hi, coef_lo, own)


def exchange(x, axes, parts):
    pieces = x.reshape(parts, -1, LANES)
    arrived = lax.all_to_all(pieces, axes, split_axis=0, concat_axis=0, tiled=True)
    return arrived.reshape(x.shape)


def local(
    tokens,
    norm_gain,
    w_query,
    w_key,
    w_value,
    query_gain,
    key_gain,
    score_bias,
    key_cache,
    value_cache,
    lengths,
    w_out,
    post_gain,
    routes,
    route_weight,
    expert_gate,
    expert_up,
    expert_down,
    shared_gate,
    shared_up,
    shared_down,
):
    small = (
        lengths,
        score_bias[None, :],
        routes.T,
        route_weight.T,
        norm_gain[None, :],
        query_gain[None, :],
    )
    late = (
        post_gain[None, :],
        expert_gate[0],
        expert_up[0],
        expert_down[0],
        shared_gate.T,
        shared_up.T,
        shared_down,
        w_key,
        w_value,
        key_gain[None, :],
    )
    partial_rows, normed, tok_slice, pick, coef_hi, coef_lo, *late = attention(
        small, tokens, w_query, key_cache, value_cache, w_out, late
    )
    arrived = exchange(partial_rows, ("ta", "tb"), TA * TB)
    outgoing, own = dispatch(arrived, tok_slice, pick)
    received = exchange(outgoing, ("ep", "tb"), EP * TB)
    parts, new_keys, new_values = run_experts(received, normed, *late)
    returned = exchange(parts, ("ep", "ta", "tb"), EP * TA * TB)
    mixed = combine(returned, coef_hi, coef_lo, own)
    return (mixed, new_keys, new_values)


def solution(mesh):
    cut = Mesh(mesh.devices.reshape(EP, TA, TB), ("ep", "ta", "tb"))
    tp = ("ta", "tb")
    placed = (
        P("ep", None),
        P(),
        P(None, tp),
        P(None, tp),
        P(None, tp),
        P(),
        P(),
        P(tp),
        P("ep", None, tp),
        P("ep", None, tp),
        P("ep"),
        P(tp, None),
        P(),
        P("ep", None),
        P("ep", None),
        P(("ep", "ta", "tb"), None, None),
        P(("ep", "ta", "tb"), None, None),
        P(("ep", "ta", "tb"), None, None),
        P(None, tp),
        P(None, tp),
        P(tp, None),
    )
    return jax.shard_map(
        local,
        mesh=cut,
        in_specs=placed,
        out_specs=(P("ep", tp),) * 3,
        check_vma=False,
    )
```

```python
import jax
import jax.numpy as jnp
from jax import lax
from jax.experimental import pallas as pl
from jax.experimental.pallas import tpu as pltpu
from jax.sharding import Mesh, PartitionSpec as P

EPS = 1e-06
BF16 = jnp.bfloat16
F32 = jnp.float32
LANES = 128
EP, TA, TB = 16, 4, 4
ROWS = 16
SLOTS = 4
LATE = 7
BLOCKS = 16
MIB = 1024 * 1024


def rms_rows(values, gain):
    mean_sq = jnp.mean(values * values, axis=-1, keepdims=True)
    return values * lax.rsqrt(mean_sq + EPS) * gain


def dot(x, w):
    return jnp.dot(x, w, preferred_element_type=F32)


def dot_nt(x, w):
    return lax.dot_general(x, w, (((1,), (1,)), ((), ())), preferred_element_type=F32)


def vmem():
    return pl.BlockSpec(memory_space=pltpu.VMEM)


def hbm():
    return pl.BlockSpec(memory_space=pltpu.HBM)


def route_tables(routes, weights, a, pick_ref, coef_hi_ref, coef_lo_ref):
    experts = EP * TA
    expert_ids = lax.broadcasted_iota(jnp.int32, (experts, ROWS), 0)
    member = jnp.zeros((experts, ROWS), F32)
    weight_of = jnp.zeros((experts, ROWS), F32)
    for k in range(routes.shape[0]):
        hit = routes[k : k + 1, :] == expert_ids
        member = member + jnp.where(hit, 1.0, 0.0)
        weight_of = weight_of + jnp.where(hit, weights[k : k + 1, :], 0.0)
    row_in = lax.broadcasted_iota(jnp.int32, (ROWS, ROWS), 0)
    row_out = lax.broadcasted_iota(jnp.int32, (ROWS, ROWS), 1)
    rank = dot(member.astype(BF16), (row_in < row_out).astype(F32).astype(BF16))
    slot_of = (member * (rank + 1.0)).astype(BF16)

    count = EP * TB * TA * SLOTS
    wide_in = lax.broadcasted_iota(jnp.int32, (ROWS, 64), 0)
    wide_out = lax.broadcasted_iota(jnp.int32, (ROWS, 64), 1)
    widen = (wide_out % ROWS == wide_in).astype(F32).astype(BF16)
    row = lax.broadcasted_iota(jnp.int32, (count, 64), 0)
    lane = lax.broadcasted_iota(jnp.int32, (count, 64), 1)
    owner = (lane == (row // 64) * TA + a).astype(F32).astype(BF16)
    found = dot(owner, dot(slot_of, widen).astype(BF16))
    slot = row % SLOTS
    same_block = (row // SLOTS) % TA == lane // ROWS
    routed = found == (slot + 1).astype(F32)
    shared = lane % ROWS == row // 64
    chosen = jnp.where(slot == SLOTS - 1, shared.astype(F32), routed.astype(F32))
    pick_ref[...] = jnp.where(same_block, chosen, 0.0).astype(BF16)

    turn = (row_in == row_out).astype(F32).astype(BF16)
    spread_row = lax.broadcasted_iota(jnp.int32, (experts, count), 0)
    spread_lane = lax.broadcasted_iota(jnp.int32, (experts, count), 1)
    spread = (spread_row == spread_lane // 16).astype(F32).astype(BF16)
    hi = weight_of.astype(BF16)
    lo = (weight_of - hi.astype(F32)).astype(BF16)
    turned = dot_nt(turn, jnp.concatenate([slot_of, hi, lo], axis=0)).astype(BF16)
    by_col = dot(
        jnp.concatenate([turned[:, n * experts : (n + 1) * experts] for n in range(3)], axis=0),
        spread,
    )
    col = lax.broadcasted_iota(jnp.int32, (ROWS, count), 1)
    token = lax.broadcasted_iota(jnp.int32, (ROWS, count), 0)
    col_slot = col % SLOTS
    held = by_col[:ROWS] == (col_slot + 1).astype(F32)
    is_shared = col_slot == SLOTS - 1
    own_shared = (token == col // 64).astype(F32)
    coef_hi_ref[...] = jnp.where(
        is_shared, own_shared, jnp.where(held, by_col[ROWS : 2 * ROWS], 0.0)
    ).astype(BF16)
    coef_lo_ref[...] = jnp.where(is_shared | ~held, 0.0, by_col[2 * ROWS :]).astype(BF16)


def attention_kernel(
    bias_hbm,
    lengths_hbm,
    norm_gain_hbm,
    query_gain_hbm,
    key_gain_hbm,
    routes_hbm,
    route_weight_hbm,
    tokens_hbm,
    wq_hbm,
    wk_hbm,
    wv_hbm,
    key_hbm,
    value_hbm,
    wout_hbm,
    *rest,
):
    late_hbm, rest = rest[:LATE], rest[LATE:]
    (
    out_ref,
    new_keys_hbm,
    new_values_hbm,
    tok_slice_ref,
    pick_ref,
    coef_hi_ref,
    coef_lo_ref,
    *rest,
    ) = rest
    late_refs, rest = rest[:LATE], rest[LATE:]
    (
    bias_buf,
    lengths_buf,
    norm_gain_buf,
    query_gain_buf,
    key_gain_buf,
    routes_buf,
    route_weight_buf,
    tokens_buf,
    wq_buf,
    wk_buf,
    wv_buf,
    key_buf,
    value_buf,
    wout_buf,
    q_buf,
    z_buf,
    w_buf,
    att_buf,
    length_rows,
    new_keys_buf,
    new_values_buf,
    small_sem,
    sem,
    key_sem,
    value_sem,
    out_sem,
    late_sem,
    ) = rest
    a, b = lax.axis_index("ta"), lax.axis_index("tb")
    small = [
        pltpu.make_async_copy(src, dst, small_sem.at[n])
        for n, (src, dst) in enumerate(
            (
                (lengths_hbm, lengths_buf),
                (bias_hbm, bias_buf),
                (routes_hbm, routes_buf),
                (route_weight_hbm, route_weight_buf),
                (norm_gain_hbm, norm_gain_buf),
                (query_gain_hbm, query_gain_buf),
                (key_gain_hbm, key_gain_buf),
            )
        )
    ]
    large = [
        pltpu.make_async_copy(src, dst, sem.at[n])
        for n, (src, dst) in enumerate(
            (
                (tokens_hbm, tokens_buf),
                (wq_hbm, wq_buf),
                (wk_hbm, wk_buf),
                (wv_hbm, wv_buf),
                (wout_hbm, wout_buf),
            )
        )
    ]
    late = [
        pltpu.make_async_copy(src, dst, late_sem.at[n])
        for n, (src, dst) in enumerate(zip(late_hbm, late_refs))
    ]
    cache_len = key_buf.shape[1]
    head_size = key_buf.shape[2]
    key_head = pltpu.make_async_copy(key_hbm, key_buf, key_sem.at[ROWS])
    value_copies = [pltpu.make_async_copy(value_hbm, value_buf, value_sem.at[ROWS])]
    for copy in small + large[:4] + [key_head] + value_copies + large[4:]:
        copy.start()

    for copy in small + large[:4]:
        copy.wait()
    for s in range(ROWS):
        length_rows[s : s + 1, :] = jnp.full((1, LANES), lengths_buf[s], jnp.int32)
    normed = rms_rows(tokens_buf[...].astype(F32), norm_gain_buf[...]).astype(BF16)
    q_buf[...] = (
        rms_rows(dot(normed, wq_buf[...]), query_gain_buf[...]).astype(BF16).astype(F32)
    )
    new_keys_buf[...] = rms_rows(dot(normed, wk_buf[...]), key_gain_buf[...]).astype(BF16)
    new_values_buf[...] = dot(normed, wv_buf[...]).astype(BF16)
    out_copies = [
        pltpu.make_async_copy(new_keys_buf, new_keys_hbm, out_sem.at[0]),
        pltpu.make_async_copy(new_values_buf, new_values_hbm, out_sem.at[1]),
    ]
    for copy in out_copies:
        copy.start()
    route_tables(
        routes_buf[...], route_weight_buf[...], a, pick_ref, coef_hi_ref, coef_lo_ref
    )
    for j in range(TA):
        cols = pl.ds(pl.multiple_of((j * TB + b) * LANES, LANES), LANES)
        tok_slice_ref[j * ROWS : (j + 1) * ROWS, :] = tokens_buf[:, cols].astype(F32)

    key_head.wait()
    for copy in late:
        copy.start()
    for s in range(ROWS):
        z_buf[s : s + 1, :] = dot_nt(q_buf[s : s + 1, :].astype(BF16), key_buf[s])

    chunks = cache_len // LANES
    after = lax.broadcasted_iota(jnp.int32, (3 * LANES, LANES), 0) % LANES
    upto = lax.broadcasted_iota(jnp.int32, (3 * LANES, LANES), 1)
    later = (after > upto).astype(F32).astype(BF16)
    chunk_lane = lax.broadcasted_iota(jnp.int32, (ROWS, LANES), 1)
    logits = z_buf[...] * head_size ** (-0.5) + bias_buf[0, 0]
    soft = jnp.log1p(jnp.exp(-jnp.abs(logits)))
    log_beta = jnp.minimum(logits, 0.0) - soft
    log_not = jnp.minimum(-logits, 0.0) - soft
    visible = [chunk_lane + c * LANES < length_rows[...] for c in range(chunks)]
    stacked = jnp.concatenate(
        [
            jnp.where(visible[c], log_not[:, c * LANES : (c + 1) * LANES], 0.0)
            for c in range(chunks)
        ],
        axis=0,
    )
    first = stacked.astype(BF16)
    rest = stacked - first.astype(F32)
    second = rest.astype(BF16)
    third = (rest - second.astype(F32)).astype(BF16)
    inner = dot(jnp.concatenate([first, second, third], axis=1), later)
    totals = jnp.sum(stacked, axis=1, keepdims=True)
    carry = jnp.zeros((ROWS, 1), F32)
    for c in reversed(range(chunks)):
        cols = slice(c * LANES, (c + 1) * LANES)
        later_sum = inner[c * ROWS : (c + 1) * ROWS, :] + carry
        w_buf[:, cols] = jnp.where(visible[c], jnp.exp(log_beta[:, cols] + later_sum), 0.0)
        carry = carry + totals[c * ROWS : (c + 1) * ROWS, :]

    for copy in value_copies + large[4:]:
        copy.wait()
    for s in range(ROWS):
        att_buf[s : s + 1, :] = dot(w_buf[s : s + 1, :].astype(BF16), value_buf[s])
    attn = dot(att_buf[...].astype(BF16), wout_buf[...]).astype(BF16)
    for t in range(BLOCKS):
        block = attn[:, t * LANES : (t + 1) * LANES]
        j, quarter = t // TB, t % TB
        for n in range(TA):
            start = (n * TB + quarter) * 64 + j * ROWS
            out_ref[start : start + ROWS, :] = block
    for copy in out_copies + late:
        copy.wait()


def attention(
    bias,
    lengths,
    norm_gain,
    query_gain,
    key_gain,
    routes,
    route_weight,
    tokens,
    wq,
    wk,
    wv,
    keys,
    values,
    wout,
    *late,
):
    rows, cache_len, head_size = keys.shape
    width = tokens.shape[1]
    shape = jax.ShapeDtypeStruct
    return pl.pallas_call(
        attention_kernel,
        name="attention",
        out_shape=(
            shape((1024, LANES), BF16),
            shape((rows, head_size), BF16),
            shape((rows, head_size), BF16),
            shape((64, LANES), F32),
            shape((1024, 64), BF16),
            shape((rows, 1024), BF16),
            shape((rows, 1024), BF16),
            *(shape(x.shape, x.dtype) for x in late),
        ),
        in_specs=[hbm()] * (14 + LATE),
        out_specs=(vmem(), hbm(), hbm()) + (vmem(),) * (4 + LATE),
        scratch_shapes=[
            pltpu.SMEM(bias.shape, F32),
            pltpu.SMEM(lengths.shape, jnp.int32),
            pltpu.VMEM(norm_gain.shape, F32),
            pltpu.VMEM(query_gain.shape, F32),
            pltpu.VMEM(key_gain.shape, F32),
            pltpu.VMEM(routes.shape, jnp.int32),
            pltpu.VMEM(route_weight.shape, F32),
            pltpu.VMEM((rows, width), BF16),
            pltpu.VMEM((width, head_size), BF16),
            pltpu.VMEM((width, head_size), BF16),
            pltpu.VMEM((width, head_size), BF16),
            pltpu.VMEM((rows, cache_len, head_size), BF16),
            pltpu.VMEM((rows, cache_len, head_size), BF16),
            pltpu.VMEM((head_size, width), BF16),
            pltpu.VMEM((rows, head_size), F32),
            pltpu.VMEM((rows, cache_len), F32),
            pltpu.VMEM((rows, cache_len), F32),
            pltpu.VMEM((rows, head_size), F32),
            pltpu.VMEM((rows, LANES), jnp.int32),
            pltpu.VMEM((rows, head_size), BF16),
            pltpu.VMEM((rows, head_size), BF16),
            pltpu.SemaphoreType.DMA((7,)),
            pltpu.SemaphoreType.DMA((5,)),
            pltpu.SemaphoreType.DMA((rows + 1,)),
            pltpu.SemaphoreType.DMA((rows + 1,)),
            pltpu.SemaphoreType.DMA((2,)),
            pltpu.SemaphoreType.DMA((LATE,)),
        ],
        cost_estimate=pl.CostEstimate(
            flops=2_000_000_000, bytes_accessed=10 * MIB, transcendentals=0
        ),
        compiler_params=pltpu.CompilerParams(vmem_limit_bytes=16 * MIB),
    )(
        bias,
        *(pltpu.with_memory_space_constraint(x, pltpu.HBM) for x in (
        lengths,
        norm_gain,
        query_gain,
        key_gain,
        routes,
        route_weight,
        tokens,
        wq,
        wk,
        wv,
        keys,
        values,
        wout,
        *late,
        ))
    )


def dispatch_kernel(arrived_ref, tok_slice_ref, pick_ref, out_ref, own_ref, h_buf):
    total = tok_slice_ref[...]
    parts = [arrived_ref[n * 64 : (n + 1) * 64, :].astype(F32) for n in range(TA * TB)]
    while len(parts) > 1:
        parts = [parts[n] + parts[n + 1] for n in range(0, len(parts), 2)]
    h = (total + parts[0]).astype(BF16)
    h_buf[...] = h.astype(F32)
    out_ref[...] = dot(pick_ref[...], h).astype(BF16)
    own_ref[...] = h_buf[pl.ds(pl.multiple_of(lax.axis_index("ta") * ROWS, ROWS), ROWS), :]


def dispatch(arrived, tok_slice, pick):
    shape = jax.ShapeDtypeStruct
    return pl.pallas_call(
        dispatch_kernel,
        name="dispatch",
        out_shape=(shape((1024, LANES), BF16), shape((ROWS, LANES), F32)),
        in_specs=[vmem()] * 3,
        out_specs=(vmem(),) * 2,
        scratch_shapes=[pltpu.VMEM((64, LANES), F32)],
        cost_estimate=pl.CostEstimate(
            flops=500_000_000, bytes_accessed=MIB, transcendentals=0
        ),
        compiler_params=pltpu.CompilerParams(vmem_limit_bytes=4 * MIB),
    )(arrived, tok_slice, pick)


def expert_kernel(
    arrived_ref,
    post_gain_ref,
    gate_ref,
    up_ref,
    down_ref,
    shared_gate_ref,
    shared_up_ref,
    shared_down_ref,
    out_ref,
    rows_buf,
    x_buf,
    send_buf,
):
    rows_buf[...] = arrived_ref[...].astype(F32)
    for t in range(BLOCKS):
        j, b = t // TB, t % TB
        for s in range(SLOTS):
            x_buf[s * ROWS : (s + 1) * ROWS, t * LANES : (t + 1) * LANES] = rows_buf[
                pl.ds(b * 16 + j * SLOTS + s, EP, stride=64), :
            ]
    h_normed = rms_rows(x_buf[...], post_gain_ref[...]).astype(BF16)
    routed_rows, shared_rows = h_normed[:48], h_normed[48:]
    gate = dot(routed_rows, gate_ref[...])
    up = dot(routed_rows, up_ref[...])
    hidden = (gate * jax.nn.sigmoid(gate) * up).astype(BF16)
    s_gate = dot_nt(shared_rows, shared_gate_ref[...])
    s_up = dot_nt(shared_rows, shared_up_ref[...])
    s_hidden = (s_gate * jax.nn.sigmoid(s_gate) * s_up).astype(BF16)
    routed = dot(hidden, down_ref[...])
    shared = dot(s_hidden, shared_down_ref[...])
    for t in range(BLOCKS):
        cols = slice(t * LANES, (t + 1) * LANES)
        for s in range(SLOTS):
            part = routed[s * ROWS : (s + 1) * ROWS, cols] if s < SLOTS - 1 else shared[:, cols]
            send_buf[pl.ds(t * SLOTS + s, EP, stride=64), :] = part
    out_ref[...] = send_buf[...].astype(BF16)


def run_experts(arrived, post_gain, gate, up, down, s_gate, s_up, s_down):
    return pl.pallas_call(
        expert_kernel,
        name="experts",
        out_shape=jax.ShapeDtypeStruct((1024, LANES), BF16),
        in_specs=[vmem()] * 8,
        out_specs=vmem(),
        scratch_shapes=[
            pltpu.VMEM((1024, LANES), F32),
            pltpu.VMEM((64, BLOCKS * LANES), F32),
            pltpu.VMEM((1024, LANES), F32),
        ],
        cost_estimate=pl.CostEstimate(
            flops=1_000_000_000, bytes_accessed=3 * MIB, transcendentals=0
        ),
        compiler_params=pltpu.CompilerParams(vmem_limit_bytes=12 * MIB),
    )(arrived, post_gain, gate, up, down, s_gate, s_up, s_down)


def combine_kernel(arrived_ref, coef_hi_ref, coef_lo_ref, own_ref, out_ref):
    arrived = arrived_ref[...]
    both = dot(jnp.concatenate([coef_hi_ref[...], coef_lo_ref[...]], axis=0), arrived)
    out_ref[...] = (own_ref[...] + (both[:ROWS] + both[ROWS:])).astype(BF16)


def combine(arrived, coef_hi, coef_lo, own):
    return pl.pallas_call(
        combine_kernel,
        name="combine",
        out_shape=jax.ShapeDtypeStruct((ROWS, LANES), BF16),
        in_specs=[vmem()] * 4,
        out_specs=vmem(),
        cost_estimate=pl.CostEstimate(
            flops=100_000_000, bytes_accessed=MIB, transcendentals=0
        ),
        compiler_params=pltpu.CompilerParams(vmem_limit_bytes=4 * MIB),
    )(arrived, coef_hi, coef_lo, own)


def exchange(x, axes, parts):
    pieces = x.reshape(parts, -1, LANES)
    arrived = lax.all_to_all(pieces, axes, split_axis=0, concat_axis=0, tiled=True)
    return arrived.reshape(x.shape)


def local(
    tokens,
    norm_gain,
    w_query,
    w_key,
    w_value,
    query_gain,
    key_gain,
    score_bias,
    key_cache,
    value_cache,
    lengths,
    w_out,
    post_gain,
    routes,
    route_weight,
    expert_gate,
    expert_up,
    expert_down,
    shared_gate,
    shared_up,
    shared_down,
):
    partial_rows, new_keys, new_values, tok_slice, pick, coef_hi, coef_lo, *late = attention(
        score_bias[None, :],
        lengths,
        norm_gain[None, :],
        query_gain[None, :],
        key_gain[None, :],
        routes.T,
        route_weight.T,
        tokens,
        w_query,
        w_key,
        w_value,
        key_cache,
        value_cache,
        w_out,
        post_gain[None, :],
        expert_gate[0],
        expert_up[0],
        expert_down[0],
        shared_gate.T,
        shared_up.T,
        shared_down,
    )
    arrived = exchange(partial_rows, ("ta", "tb"), TA * TB)
    outgoing, own = dispatch(arrived, tok_slice, pick)
    received = exchange(outgoing, ("ep", "tb"), EP * TB)
    parts = run_experts(received, *late)
    returned = exchange(parts, ("ep", "ta", "tb"), EP * TA * TB)
    mixed = combine(returned, coef_hi, coef_lo, own)
    return (mixed, new_keys, new_values)


def solution(mesh):
    cut = Mesh(mesh.devices.reshape(EP, TA, TB), ("ep", "ta", "tb"))
    tp = ("ta", "tb")
    placed = (
        P("ep", None),
        P(),
        P(None, tp),
        P(None, tp),
        P(None, tp),
        P(),
        P(),
        P(tp),
        P("ep", None, tp),
        P("ep", None, tp),
        P("ep"),
        P(tp, None),
        P(),
        P("ep", None),
        P("ep", None),
        P(("ep", "ta", "tb"), None, None),
        P(("ep", "ta", "tb"), None, None),
        P(("ep", "ta", "tb"), None, None),
        P(None, tp),
        P(None, tp),
        P(tp, None),
    )
    return jax.shard_map(
        local,
        mesh=cut,
        in_specs=placed,
        out_specs=(P("ep", tp),) * 3,
        check_vma=False,
    )
```

```python
import jax
import jax.numpy as jnp
from jax import lax
from jax.experimental import pallas as pl
from jax.experimental.pallas import tpu as pltpu
from jax.sharding import Mesh, PartitionSpec as P

EPS = 1e-06
BF16 = jnp.bfloat16
F32 = jnp.float32
LANES = 128
EP, TA, TB = 16, 4, 4
ROWS = 16
SLOTS = 4
LATE = 7
BLOCKS = 16
MIB = 1024 * 1024


def rms_rows(values, gain):
    mean_sq = jnp.mean(values * values, axis=-1, keepdims=True)
    return values * lax.rsqrt(mean_sq + EPS) * gain


def dot(x, w):
    return jnp.dot(x, w, preferred_element_type=F32)


def dot_nt(x, w):
    return lax.dot_general(x, w, (((1,), (1,)), ((), ())), preferred_element_type=F32)


def vmem():
    return pl.BlockSpec(memory_space=pltpu.VMEM)


def hbm():
    return pl.BlockSpec(memory_space=pltpu.HBM)


def route_tables(routes, weights, a, pick_ref, coef_hi_ref, coef_lo_ref):
    experts = EP * TA
    expert_ids = lax.broadcasted_iota(jnp.int32, (experts, ROWS), 0)
    member = jnp.zeros((experts, ROWS), F32)
    weight_of = jnp.zeros((experts, ROWS), F32)
    for k in range(routes.shape[0]):
        hit = routes[k : k + 1, :] == expert_ids
        member = member + jnp.where(hit, 1.0, 0.0)
        weight_of = weight_of + jnp.where(hit, weights[k : k + 1, :], 0.0)
    row_in = lax.broadcasted_iota(jnp.int32, (ROWS, ROWS), 0)
    row_out = lax.broadcasted_iota(jnp.int32, (ROWS, ROWS), 1)
    rank = dot(member.astype(BF16), (row_in < row_out).astype(F32).astype(BF16))
    slot_of = (member * (rank + 1.0)).astype(BF16)

    count = EP * TB * TA * SLOTS
    wide_in = lax.broadcasted_iota(jnp.int32, (ROWS, 64), 0)
    wide_out = lax.broadcasted_iota(jnp.int32, (ROWS, 64), 1)
    widen = (wide_out % ROWS == wide_in).astype(F32).astype(BF16)
    row = lax.broadcasted_iota(jnp.int32, (count, 64), 0)
    lane = lax.broadcasted_iota(jnp.int32, (count, 64), 1)
    owner = (lane == (row // 64) * TA + a).astype(F32).astype(BF16)
    found = dot(owner, dot(slot_of, widen).astype(BF16))
    slot = row % SLOTS
    same_block = (row // SLOTS) % TA == lane // ROWS
    routed = found == (slot + 1).astype(F32)
    shared = lane % ROWS == row // 64
    chosen = jnp.where(slot == SLOTS - 1, shared.astype(F32), routed.astype(F32))
    pick_ref[...] = jnp.where(same_block, chosen, 0.0).astype(BF16)

    turn = (row_in == row_out).astype(F32).astype(BF16)
    spread_row = lax.broadcasted_iota(jnp.int32, (experts, count), 0)
    spread_lane = lax.broadcasted_iota(jnp.int32, (experts, count), 1)
    spread = (spread_row == spread_lane // 16).astype(F32).astype(BF16)
    hi = weight_of.astype(BF16)
    lo = (weight_of - hi.astype(F32)).astype(BF16)
    turned = dot_nt(turn, jnp.concatenate([slot_of, hi, lo], axis=0)).astype(BF16)
    by_col = dot(
        jnp.concatenate([turned[:, n * experts : (n + 1) * experts] for n in range(3)], axis=0),
        spread,
    )
    col = lax.broadcasted_iota(jnp.int32, (ROWS, count), 1)
    token = lax.broadcasted_iota(jnp.int32, (ROWS, count), 0)
    col_slot = col % SLOTS
    held = by_col[:ROWS] == (col_slot + 1).astype(F32)
    is_shared = col_slot == SLOTS - 1
    own_shared = (token == col // 64).astype(F32)
    coef_hi_ref[...] = jnp.where(
        is_shared, own_shared, jnp.where(held, by_col[ROWS : 2 * ROWS], 0.0)
    ).astype(BF16)
    coef_lo_ref[...] = jnp.where(is_shared | ~held, 0.0, by_col[2 * ROWS :]).astype(BF16)


def attention_kernel(
    bias_hbm,
    lengths_hbm,
    norm_gain_hbm,
    query_gain_hbm,
    key_gain_hbm,
    routes_hbm,
    route_weight_hbm,
    tokens_hbm,
    wq_hbm,
    wk_hbm,
    wv_hbm,
    key_hbm,
    value_hbm,
    wout_hbm,
    *rest,
):
    late_hbm, rest = rest[:LATE], rest[LATE:]
    (out_ref, new_keys_hbm, new_values_hbm, tok_slice_ref), rest = rest[:4], rest[4:]
    (pick_ref, coef_hi_ref, coef_lo_ref), rest = rest[:3], rest[3:]
    late_refs, rest = rest[:LATE], rest[LATE:]
    (bias_buf, lengths_buf, norm_gain_buf, query_gain_buf), rest = rest[:4], rest[4:]
    (key_gain_buf, routes_buf, route_weight_buf, tokens_buf), rest = rest[:4], rest[4:]
    (wq_buf, wk_buf, wv_buf, key_buf, value_buf, wout_buf), rest = rest[:6], rest[6:]
    (q_buf, z_buf, w_buf, att_buf, length_rows), rest = rest[:5], rest[5:]
    (new_keys_buf, new_values_buf), sems = rest[:2], rest[2:]
    small_sem, sem, key_sem, value_sem, out_sem, late_sem = sems
    a, b = lax.axis_index("ta"), lax.axis_index("tb")
    small = [
        pltpu.make_async_copy(src, dst, small_sem.at[n])
        for n, (src, dst) in enumerate(
            (
                (lengths_hbm, lengths_buf),
                (bias_hbm, bias_buf),
                (routes_hbm, routes_buf),
                (route_weight_hbm, route_weight_buf),
                (norm_gain_hbm, norm_gain_buf),
                (query_gain_hbm, query_gain_buf),
                (key_gain_hbm, key_gain_buf),
            )
        )
    ]
    large = [
        pltpu.make_async_copy(src, dst, sem.at[n])
        for n, (src, dst) in enumerate(
            (
                (tokens_hbm, tokens_buf),
                (wq_hbm, wq_buf),
                (wk_hbm, wk_buf),
                (wv_hbm, wv_buf),
                (wout_hbm, wout_buf),
            )
        )
    ]
    late = [
        pltpu.make_async_copy(src, dst, late_sem.at[n])
        for n, (src, dst) in enumerate(zip(late_hbm, late_refs))
    ]
    cache_len = key_buf.shape[1]
    head_size = key_buf.shape[2]
    key_copy = pltpu.make_async_copy(key_hbm, key_buf, key_sem.at[0])
    value_copy = pltpu.make_async_copy(value_hbm, value_buf, value_sem.at[0])
    for copy in small + large[:4] + [key_copy, value_copy] + large[4:]:
        copy.start()

    for copy in small + large[:4]:
        copy.wait()
    for s in range(ROWS):
        length_rows[s : s + 1, :] = jnp.full((1, LANES), lengths_buf[s], jnp.int32)
    normed = rms_rows(tokens_buf[...].astype(F32), norm_gain_buf[...]).astype(BF16)
    q_buf[...] = (
        rms_rows(dot(normed, wq_buf[...]), query_gain_buf[...]).astype(BF16).astype(F32)
    )
    new_keys_buf[...] = rms_rows(dot(normed, wk_buf[...]), key_gain_buf[...]).astype(BF16)
    new_values_buf[...] = dot(normed, wv_buf[...]).astype(BF16)
    out_copies = [
        pltpu.make_async_copy(new_keys_buf, new_keys_hbm, out_sem.at[0]),
        pltpu.make_async_copy(new_values_buf, new_values_hbm, out_sem.at[1]),
    ]
    for copy in out_copies:
        copy.start()
    route_tables(
        routes_buf[...], route_weight_buf[...], a, pick_ref, coef_hi_ref, coef_lo_ref
    )
    for j in range(TA):
        cols = pl.ds(pl.multiple_of((j * TB + b) * LANES, LANES), LANES)
        tok_slice_ref[j * ROWS : (j + 1) * ROWS, :] = tokens_buf[:, cols].astype(F32)

    key_copy.wait()
    for copy in late:
        copy.start()
    for s in range(ROWS):
        z_buf[s : s + 1, :] = dot_nt(q_buf[s : s + 1, :].astype(BF16), key_buf[s])

    chunks = cache_len // LANES
    after = lax.broadcasted_iota(jnp.int32, (3 * LANES, LANES), 0) % LANES
    upto = lax.broadcasted_iota(jnp.int32, (3 * LANES, LANES), 1)
    later = (after > upto).astype(F32).astype(BF16)
    chunk_lane = lax.broadcasted_iota(jnp.int32, (ROWS, LANES), 1)
    logits = z_buf[...] * head_size ** (-0.5) + bias_buf[0, 0]
    soft = jnp.log1p(jnp.exp(-jnp.abs(logits)))
    log_beta = jnp.minimum(logits, 0.0) - soft
    log_not = jnp.minimum(-logits, 0.0) - soft
    visible = [chunk_lane + c * LANES < length_rows[...] for c in range(chunks)]
    stacked = jnp.concatenate(
        [
            jnp.where(visible[c], log_not[:, c * LANES : (c + 1) * LANES], 0.0)
            for c in range(chunks)
        ],
        axis=0,
    )
    first = stacked.astype(BF16)
    rest = stacked - first.astype(F32)
    second = rest.astype(BF16)
    third = (rest - second.astype(F32)).astype(BF16)
    inner = dot(jnp.concatenate([first, second, third], axis=1), later)
    totals = jnp.sum(stacked, axis=1, keepdims=True)
    carry = jnp.zeros((ROWS, 1), F32)
    for c in reversed(range(chunks)):
        cols = slice(c * LANES, (c + 1) * LANES)
        later_sum = inner[c * ROWS : (c + 1) * ROWS, :] + carry
        w_buf[:, cols] = jnp.where(visible[c], jnp.exp(log_beta[:, cols] + later_sum), 0.0)
        carry = carry + totals[c * ROWS : (c + 1) * ROWS, :]

    for copy in [value_copy] + large[4:]:
        copy.wait()
    for s in range(ROWS):
        att_buf[s : s + 1, :] = dot(w_buf[s : s + 1, :].astype(BF16), value_buf[s])
    attn = dot(att_buf[...].astype(BF16), wout_buf[...]).astype(BF16)
    for t in range(BLOCKS):
        block = attn[:, t * LANES : (t + 1) * LANES]
        j, quarter = t // TB, t % TB
        for n in range(TA):
            start = (n * TB + quarter) * 64 + j * ROWS
            out_ref[start : start + ROWS, :] = block
    for copy in out_copies + late:
        copy.wait()


def attention(
    bias,
    lengths,
    norm_gain,
    query_gain,
    key_gain,
    routes,
    route_weight,
    tokens,
    wq,
    wk,
    wv,
    keys,
    values,
    wout,
    *late,
):
    rows, cache_len, head_size = keys.shape
    width = tokens.shape[1]
    shape = jax.ShapeDtypeStruct
    return pl.pallas_call(
        attention_kernel,
        name="attention",
        out_shape=(
            shape((1024, LANES), BF16),
            shape((rows, head_size), BF16),
            shape((rows, head_size), BF16),
            shape((64, LANES), F32),
            shape((1024, 64), BF16),
            shape((rows, 1024), BF16),
            shape((rows, 1024), BF16),
            *(shape(x.shape, x.dtype) for x in late),
        ),
        in_specs=[hbm()] * (14 + LATE),
        out_specs=(vmem(), hbm(), hbm()) + (vmem(),) * (4 + LATE),
        scratch_shapes=[
            pltpu.SMEM(bias.shape, F32),
            pltpu.SMEM(lengths.shape, jnp.int32),
            pltpu.VMEM(norm_gain.shape, F32),
            pltpu.VMEM(query_gain.shape, F32),
            pltpu.VMEM(key_gain.shape, F32),
            pltpu.VMEM(routes.shape, jnp.int32),
            pltpu.VMEM(route_weight.shape, F32),
            pltpu.VMEM((rows, width), BF16),
            pltpu.VMEM((width, head_size), BF16),
            pltpu.VMEM((width, head_size), BF16),
            pltpu.VMEM((width, head_size), BF16),
            pltpu.VMEM((rows, cache_len, head_size), BF16),
            pltpu.VMEM((rows, cache_len, head_size), BF16),
            pltpu.VMEM((head_size, width), BF16),
            pltpu.VMEM((rows, head_size), F32),
            pltpu.VMEM((rows, cache_len), F32),
            pltpu.VMEM((rows, cache_len), F32),
            pltpu.VMEM((rows, head_size), F32),
            pltpu.VMEM((rows, LANES), jnp.int32),
            pltpu.VMEM((rows, head_size), BF16),
            pltpu.VMEM((rows, head_size), BF16),
            pltpu.SemaphoreType.DMA((7,)),
            pltpu.SemaphoreType.DMA((5,)),
            pltpu.SemaphoreType.DMA((1,)),
            pltpu.SemaphoreType.DMA((1,)),
            pltpu.SemaphoreType.DMA((2,)),
            pltpu.SemaphoreType.DMA((LATE,)),
        ],
        cost_estimate=pl.CostEstimate(
            flops=2_000_000_000, bytes_accessed=10 * MIB, transcendentals=0
        ),
        compiler_params=pltpu.CompilerParams(vmem_limit_bytes=16 * MIB),
    )(
        bias,
        *(
            pltpu.with_memory_space_constraint(x, pltpu.HBM)
            for x in (
                lengths,
                norm_gain,
                query_gain,
                key_gain,
                routes,
                route_weight,
                tokens,
                wq,
                wk,
                wv,
                keys,
                values,
                wout,
                *late,
            )
        ),
    )


def dispatch_kernel(arrived_ref, tok_slice_ref, pick_ref, out_ref, own_ref, h_buf):
    total = tok_slice_ref[...]
    parts = [arrived_ref[n * 64 : (n + 1) * 64, :].astype(F32) for n in range(TA * TB)]
    while len(parts) > 1:
        parts = [parts[n] + parts[n + 1] for n in range(0, len(parts), 2)]
    h = (total + parts[0]).astype(BF16)
    h_buf[...] = h.astype(F32)
    out_ref[...] = dot(pick_ref[...], h).astype(BF16)
    own_ref[...] = h_buf[pl.ds(pl.multiple_of(lax.axis_index("ta") * ROWS, ROWS), ROWS), :]


def dispatch(arrived, tok_slice, pick):
    shape = jax.ShapeDtypeStruct
    return pl.pallas_call(
        dispatch_kernel,
        name="dispatch",
        out_shape=(shape((1024, LANES), BF16), shape((ROWS, LANES), F32)),
        in_specs=[vmem()] * 3,
        out_specs=(vmem(),) * 2,
        scratch_shapes=[pltpu.VMEM((64, LANES), F32)],
        cost_estimate=pl.CostEstimate(
            flops=500_000_000, bytes_accessed=MIB, transcendentals=0
        ),
        compiler_params=pltpu.CompilerParams(vmem_limit_bytes=4 * MIB),
    )(arrived, tok_slice, pick)


def expert_kernel(
    arrived_ref,
    post_gain_ref,
    gate_ref,
    up_ref,
    down_ref,
    shared_gate_ref,
    shared_up_ref,
    shared_down_ref,
    out_ref,
    rows_buf,
    x_buf,
    send_buf,
):
    count = arrived_ref.shape[0]
    rows_buf[:count, :] = arrived_ref[...].astype(F32)
    for t in range(BLOCKS):
        j, b = t // TB, t % TB
        for s in range(SLOTS):
            x_buf[s * ROWS : (s + 1) * ROWS, t * LANES : (t + 1) * LANES] = rows_buf[
                pl.ds(b * 16 + j * SLOTS + s, EP, stride=64), :
            ]
    h_normed = rms_rows(x_buf[...], post_gain_ref[...]).astype(BF16)
    routed_rows, shared_rows = h_normed[:48], h_normed[48:]
    gate = dot(routed_rows, gate_ref[...])
    up = dot(routed_rows, up_ref[...])
    hidden = (gate * jax.nn.sigmoid(gate) * up).astype(BF16)
    s_gate = dot_nt(shared_rows, shared_gate_ref[...])
    s_up = dot_nt(shared_rows, shared_up_ref[...])
    s_hidden = (s_gate * jax.nn.sigmoid(s_gate) * s_up).astype(BF16)
    routed = dot(hidden, down_ref[...])
    shared = dot(s_hidden, shared_down_ref[...])
    for t in range(BLOCKS):
        cols = slice(t * LANES, (t + 1) * LANES)
        for s in range(SLOTS):
            part = routed[s * ROWS : (s + 1) * ROWS, cols] if s < SLOTS - 1 else shared[:, cols]
            send_buf[pl.ds(t * SLOTS + s, EP, stride=64), :] = part
    out_ref[...] = send_buf[:count, :].astype(BF16)


def run_experts(arrived, post_gain, gate, up, down, s_gate, s_up, s_down):
    return pl.pallas_call(
        expert_kernel,
        name="experts",
        out_shape=jax.ShapeDtypeStruct((1024, LANES), BF16),
        in_specs=[vmem()] * 8,
        out_specs=vmem(),
        scratch_shapes=[
            pltpu.VMEM((1024 + 64, LANES), F32),
            pltpu.VMEM((64, BLOCKS * LANES), F32),
            pltpu.VMEM((1024 + 64, LANES), F32),
        ],
        cost_estimate=pl.CostEstimate(
            flops=1_000_000_000, bytes_accessed=3 * MIB, transcendentals=0
        ),
        compiler_params=pltpu.CompilerParams(vmem_limit_bytes=12 * MIB),
    )(arrived, post_gain, gate, up, down, s_gate, s_up, s_down)


def combine_kernel(arrived_ref, coef_hi_ref, coef_lo_ref, own_ref, out_ref):
    arrived = arrived_ref[...]
    both = dot(jnp.concatenate([coef_hi_ref[...], coef_lo_ref[...]], axis=0), arrived)
    out_ref[...] = (own_ref[...] + (both[:ROWS] + both[ROWS:])).astype(BF16)


def combine(arrived, coef_hi, coef_lo, own):
    return pl.pallas_call(
        combine_kernel,
        name="combine",
        out_shape=jax.ShapeDtypeStruct((ROWS, LANES), BF16),
        in_specs=[vmem()] * 4,
        out_specs=vmem(),
        cost_estimate=pl.CostEstimate(
            flops=100_000_000, bytes_accessed=MIB, transcendentals=0
        ),
        compiler_params=pltpu.CompilerParams(vmem_limit_bytes=4 * MIB),
    )(arrived, coef_hi, coef_lo, own)


def exchange(x, axes, parts):
    pieces = x.reshape(parts, -1, LANES)
    arrived = lax.all_to_all(pieces, axes, split_axis=0, concat_axis=0, tiled=True)
    return arrived.reshape(x.shape)


def local(
    tokens,
    norm_gain,
    w_query,
    w_key,
    w_value,
    query_gain,
    key_gain,
    score_bias,
    key_cache,
    value_cache,
    lengths,
    w_out,
    post_gain,
    routes,
    route_weight,
    expert_gate,
    expert_up,
    expert_down,
    shared_gate,
    shared_up,
    shared_down,
):
    partial_rows, new_keys, new_values, tok_slice, pick, coef_hi, coef_lo, *late = attention(
        score_bias[None, :],
        lengths,
        norm_gain[None, :],
        query_gain[None, :],
        key_gain[None, :],
        routes.T,
        route_weight.T,
        tokens,
        w_query,
        w_key,
        w_value,
        key_cache,
        value_cache,
        w_out,
        post_gain[None, :],
        expert_gate[0],
        expert_up[0],
        expert_down[0],
        shared_gate.T,
        shared_up.T,
        shared_down,
    )
    arrived = exchange(partial_rows, ("ta", "tb"), TA * TB)
    outgoing, own = dispatch(arrived, tok_slice, pick)
    received = exchange(outgoing, ("ep", "tb"), EP * TB)
    parts = run_experts(received, *late)
    returned = exchange(parts, ("ep", "ta", "tb"), EP * TA * TB)
    mixed = combine(returned, coef_hi, coef_lo, own)
    return (mixed, new_keys, new_values)


def solution(mesh):
    cut = Mesh(mesh.devices.reshape(EP, TA, TB), ("ep", "ta", "tb"))
    tp = ("ta", "tb")
    placed = (
        P("ep", None),
        P(),
        P(None, tp),
        P(None, tp),
        P(None, tp),
        P(),
        P(),
        P(tp),
        P("ep", None, tp),
        P("ep", None, tp),
        P("ep"),
        P(tp, None),
        P(),
        P("ep", None),
        P("ep", None),
        P(("ep", "ta", "tb"), None, None),
        P(("ep", "ta", "tb"), None, None),
        P(("ep", "ta", "tb"), None, None),
        P(None, tp),
        P(None, tp),
        P(tp, None),
    )
    return jax.shard_map(
        local,
        mesh=cut,
        in_specs=placed,
        out_specs=(P("ep", tp),) * 3,
        check_vma=False,
    )
```
